512 devices in a mesh: fs: 64 (over z, y), tp: 8 (over x, core).
Axes of the slice: x: 4, y: 4, z: 16, core: 2. Of those that a mesh axis runs over, the one named last changes fastest.
Arguments:
- tokens: bfloat16 [20480, 2048], P('fs'), may hold values from -6 to 6
- w_gate: bfloat16 [2048, 5632], P('fs', 'tp'), may hold values from -0.125 to 0.125
- w_up: bfloat16 [2048, 5632], P('fs', 'tp'), may hold values from -0.125 to 0.125
- w_down: bfloat16 [5632, 2048], P('tp', 'fs'), may hold values from -0.078125 to 0.078125
- w_mix_in: bfloat16 [2048, 1024], P('fs', 'tp'), may hold values from -0.125 to 0.125
- w_mix_out: bfloat16 [1024, 2048], P('tp', 'fs'), may hold values from -0.1875 to 0.1875
- pool_w: bfloat16 [8, 128, 128], P('tp'), may hold values from -0.5 to 0.5
- pool_scale: bfloat16 [1024], P('tp'), may hold values from 0.099609375 to 1.8984375
- norm_gains: float32 [6, 2048], replicated, may hold values from 0.1 to 1.9
Outputs:
- layer_out: bfloat16 [20480, 2048], P(('fs', 'tp'))
The draws below stay inside these ranges and needn't reach their ends.
All inputs are finite; a program needn't handle non-finite values.
Results may differ from the reference program's by a relative error of at most 0.018.
Values may be sent and summed in bfloat16 or wider, within the bound.
No kernel may reach another device: no remote copies, remote signals or barrier semaphores. Data moves between devices by JAX's collectives and lax.ppermute only.
A program may use at most 64 MiB of HBM per device.

```python
import jax
import jax.numpy as jnp
from jax import lax

D = 2048
FF = 5632
GD = 128
NGROUP = 8
POOLW = 1024
LEN = 64
TOKENS = 20480
N_TP = 8


def levels(stream_key, shape, pieces, least, high):
    level, own = 1.0, jax.random.fold_in(stream_key, 6)
    for axis_at, parts in pieces:
        draws = jnp.exp(jax.random.uniform(jax.random.fold_in(own, axis_at), (parts,), jnp.float32, least / len(pieces), high / len(pieces)))
        level = level * jnp.repeat(draws, shape[axis_at] // parts).reshape([-1 if axis == axis_at else 1 for axis in range(len(shape))])
    return level


def bell_draw(own_key, shape, spread, most, pieces=(), kind=jnp.bfloat16):
    array = jax.random.normal(own_key, shape, jnp.float32) * spread
    if len(pieces) > 0:
        array = levels(own_key, shape, pieces, -0.22, 0.18) * array
    return jnp.clip(array, min=-most, max=most).astype(kind)


def setup_inputs(seed: int = 0) -> dict:
    key_list = jax.random.split(jax.random.key(seed), 10)
    return {
        "tokens": bell_draw(key_list[0], (TOKENS, D), 1.0, 6.0, ((0, 64),)),
        "w_gate": bell_draw(key_list[1], (D, FF), D ** -0.5, 0.125, ((0, 64), (1, 8))),
        "w_up": bell_draw(key_list[2], (D, FF), D ** -0.5, 0.125, ((0, 64), (1, 8))),
        "w_down": bell_draw(key_list[3], (FF, D), FF ** -0.5, 0.078125, ((0, 8), (1, 64))),
        "w_mix_in": bell_draw(key_list[4], (D, POOLW), D ** -0.5, 0.125, ((0, 64), (1, 8))),
        "w_mix_out": bell_draw(key_list[5], (POOLW, D), POOLW ** -0.5, 0.1875, ((0, 8), (1, 64))),
        "pool_w": bell_draw(key_list[6], (NGROUP, GD, GD), GD ** -0.5, 0.5, ((0, 8),)),
        "pool_scale": jnp.clip(1.0 + 0.18 * jax.random.normal(key_list[7], (POOLW,), jnp.float32), 0.099609375, 1.8984375).astype(jnp.bfloat16),
        "norm_gains": jnp.clip(1.0 + 0.18 * jax.random.normal(key_list[8], (6, D), jnp.float32), 0.1, 1.9),
    }


def rms_scale(values, gain):
    return values * lax.rsqrt(lax.optimization_barrier(jnp.mean(values * values, axis=-1, keepdims=True)) + 1e-06) * gain

def split_sum(left_rows, right_matrix):
    block_width = left_rows.shape[1] // N_TP

    def add_block(block_id, running_sum):
        offset = (block_id * block_width).astype(jnp.int32)
        left_part = lax.dynamic_slice_in_dim(left_rows, offset, block_width, 1)
        right_part = lax.dynamic_slice_in_dim(right_matrix, offset, block_width, 0)
        partial_value = jnp.dot(left_part, right_part, preferred_element_type=jnp.float32).astype(jnp.bfloat16)
        partial_value = lax.optimization_barrier(partial_value)
        return running_sum + partial_value.astype(jnp.float32)
    initial = jnp.zeros((left_rows.shape[0], right_matrix.shape[1]), jnp.float32)
    return lax.fori_loop(0, N_TP, add_block, initial)

def gated(normed, w_gate, w_up):
    gate_part = jnp.dot(normed, w_gate, preferred_element_type=jnp.float32)
    up_part = jnp.dot(normed, w_up, preferred_element_type=jnp.float32)
    return (jax.nn.silu(gate_part) * up_part).astype(jnp.bfloat16)

def pool_mix(pooled_in, pool_w, pool_scale):
    values = pooled_in.astype(jnp.float32).reshape(-1, LEN, NGROUP, GD)
    totals = jnp.cumsum(values, axis=1)
    position = jnp.arange(1, LEN + 1).astype(jnp.float32)[None, :, None]
    averages = []
    for group_id in range(NGROUP):
        window = 2 ** (1 + group_id % 4)
        running = totals[:, :, group_id]
        lagged = jnp.pad(running, ((0, 0), (window, 0), (0, 0)))[:, :LEN]
        averages.append((running - lagged) / jnp.minimum(position, float(window)))
    average = jnp.stack(averages, axis=2)
    deviation = (average - values).astype(jnp.bfloat16)
    regrouped = jnp.einsum('btgi,gio->btgo', deviation.astype(jnp.float32), pool_w.astype(jnp.float32))
    regrouped = regrouped.reshape(-1, NGROUP * GD) * pool_scale.astype(jnp.float32)
    return regrouped.astype(jnp.bfloat16)

def reference(tokens, w_gate, w_up, w_down, w_mix_in, w_mix_out, pool_w, pool_scale, norm_gains):
    scales = norm_gains.astype(jnp.float32)
    stream = tokens.astype(jnp.float32)
    normed = rms_scale(stream, scales[0]).astype(jnp.bfloat16)
    stream = stream + 0.5 * rms_scale(split_sum(gated(normed, w_gate, w_up), w_down), scales[1])
    normed = rms_scale(stream, scales[2]).astype(jnp.bfloat16)
    pooled_in = jnp.dot(normed, w_mix_in, preferred_element_type=jnp.float32).astype(jnp.bfloat16)
    stream = stream + rms_scale(split_sum(pool_mix(pooled_in, pool_w, pool_scale), w_mix_out), scales[3])
    normed = rms_scale(stream, scales[4]).astype(jnp.bfloat16)
    stream = stream + 0.5 * rms_scale(split_sum(gated(normed, w_gate, w_up), w_down), scales[5])
    return stream.astype(jnp.bfloat16)
```

```python
import functools

import jax
import jax.numpy as jnp
from jax import lax
from jax.experimental import pallas as pl
from jax.experimental.pallas import tpu as pltpu
from jax.sharding import PartitionSpec as P


LEN = 64
NZ, NY = 16, 4
BF = jnp.bfloat16
F32 = jnp.float32
VMEM = pl.BlockSpec(memory_space=pltpu.VMEM)
SMEM = pl.BlockSpec(memory_space=pltpu.SMEM)
LIMIT = pltpu.CompilerParams(vmem_limit_bytes=48 * 1024 * 1024)

OFFSETS = tuple(range(-8, 8))
BATCHES = ((0, -1, 1, -2, 2, -3, 3, -4, 4), (-5, 5, -6, 6, -7, 7, -8))


def fs_shift(dy, dz):
    return [
        (z * NY + y, ((z + dz) % NZ) * NY + (y + dy) % NY) for z in range(NZ) for y in range(NY)
    ]


def shift(array, dy=0, dz=0):
    return lax.ppermute(array, "fs", fs_shift(dy, dz))


def rolled(array, first_block):
    twice = jnp.concatenate([array, array], axis=1)
    return lax.dynamic_slice_in_dim(twice, first_block * 128, array.shape[1], 1)


def gated_kernel(width, x_ref, *refs):
    payloads, out_ref, w_ref = refs[:NZ], refs[NZ], refs[NZ + 1]
    for k in range(NZ):
        w_ref[k * 128 : (k + 1) * 128, :] = payloads[k][0:128, :]
    x = x_ref[...]
    whole = width // 128 * 128

    def act(gate, up):
        return (gate / (1.0 + jnp.exp(-gate)) * up).astype(BF)

    at = 0
    while at < whole:
        n = min(256, whole - at)
        gate = jnp.dot(x, w_ref[:, at : at + n], preferred_element_type=F32)
        up = jnp.dot(x, w_ref[:, whole + at : whole + at + n], preferred_element_type=F32)
        out_ref[:, at : at + n] = act(gate, up)
        at += n
    if width > whole:
        rest = width - whole
        both = jnp.dot(x, w_ref[:, 2 * whole :], preferred_element_type=F32)
        out_ref[:, whole:] = act(both[:, :rest], both[:, rest:])


def gated(x, payloads, width):
    rows, depth = x.shape
    return pl.pallas_call(
        functools.partial(gated_kernel, width),
        out_shape=jax.ShapeDtypeStruct((rows, width), BF),
        in_specs=[VMEM] * (1 + NZ),
        out_specs=VMEM,
        scratch_shapes=[pltpu.VMEM((depth, 2 * width), BF)],
        compiler_params=LIMIT,
        cost_estimate=pl.CostEstimate(
            flops=4 * rows * depth * width, bytes_accessed=8 << 20, transcendentals=0
        ),
        name="gated",
    )(x, *payloads)


def assemble_kernel(y_ref, *refs):
    ins, mix_ref, down_ref = refs[:-2], refs[-2], refs[-1]
    y = y_ref[0]
    at = 0
    for batch in BATCHES:
        for j in range(NY):
            src = ins[at]
            at += 1
            owner = lax.rem(y - j + NY, NY)
            for i, offset in enumerate(batch):
                start = pl.multiple_of(OFFSETS.index(offset) * 128 + owner * 32, 32)
                mix_ref[pl.ds(start, 32), :] = src[i * 32 : (i + 1) * 32, 0:256]
                down_ref[pl.ds(start, 32), :] = src[i * 32 : (i + 1) * 32, 256:]


def assemble(y, pieces, down_width):
    rows = NZ * NY * 32
    return pl.pallas_call(
        assemble_kernel,
        out_shape=(
            jax.ShapeDtypeStruct((rows, 256), BF),
            jax.ShapeDtypeStruct((rows, down_width), BF),
        ),
        in_specs=[SMEM] + [VMEM] * len(pieces),
        out_specs=(VMEM, VMEM),
        compiler_params=LIMIT,
        cost_estimate=pl.CostEstimate(flops=10**8, bytes_accessed=8 << 20, transcendentals=0),
        name="assemble",
    )(y, *pieces)


def down_kernel(h_ref, w_ref, out_ref):
    h = h_ref[...]
    for at in range(0, w_ref.shape[0], 256):
        out_ref[:, at : at + 256] = lax.dot_general(
            h, w_ref[at : at + 256, :], (((1,), (1,)), ((), ())), preferred_element_type=F32
        ).astype(BF)


def down(hidden, w):
    rows, out = hidden.shape[0], w.shape[0]
    return pl.pallas_call(
        down_kernel,
        out_shape=jax.ShapeDtypeStruct((rows, out), BF),
        in_specs=[VMEM, VMEM],
        out_specs=VMEM,
        compiler_params=LIMIT,
        cost_estimate=pl.CostEstimate(
            flops=2 * rows * out * w.shape[1], bytes_accessed=4 << 20, transcendentals=0
        ),
        name="down",
    )(hidden, w)


def mixer_kernel(kind_ref, x_ref, w_ref, pool_ref, scale_ref, out_ref):
    rows = x_ref.shape[0]
    kind = kind_ref[0]
    values = jnp.dot(x_ref[...], w_ref[:, 0:128], preferred_element_type=F32)
    values = values.astype(BF).astype(F32)
    place = lax.broadcasted_iota(jnp.int32, (rows, 128), 0) % LEN
    total = values
    chosen = jnp.zeros_like(values)
    for slot in range(4):
        lag = 2**slot
        earlier = jnp.concatenate([jnp.zeros((lag, 128), F32), total[: rows - lag]], axis=0)
        total = total + jnp.where(place >= lag, earlier, 0.0)
        window = 2 * lag
        mean = total / jnp.minimum(place + 1, window).astype(F32)
        chosen = jnp.where(kind == slot, mean, chosen)
    deviation = (chosen - values).astype(BF)
    mixed = jnp.dot(deviation, pool_ref[...], preferred_element_type=F32)
    mixed = (mixed * scale_ref[...].astype(F32)).astype(BF)
    for at in range(0, w_ref.shape[0], 256):
        out_ref[:, at : at + 256] = lax.dot_general(
            mixed, w_ref[at : at + 256, 128:256], (((1,), (1,)), ((), ())), preferred_element_type=F32
        ).astype(BF)


def mixer(kind, x, w, pool_w, pool_scale):
    rows, depth = x.shape
    return pl.pallas_call(
        mixer_kernel,
        out_shape=jax.ShapeDtypeStruct((rows, depth), BF),
        in_specs=[SMEM] + [VMEM] * 4,
        out_specs=VMEM,
        compiler_params=LIMIT,
        cost_estimate=pl.CostEstimate(
            flops=4 * rows * depth * 128, bytes_accessed=4 << 20, transcendentals=0
        ),
        name="mixer",
    )(kind, x, w, pool_w, pool_scale)


def rms_scale(values, gain):
    return values * lax.rsqrt(jnp.mean(values * values, axis=-1, keepdims=True) + 1e-06) * gain


def sum_at_owner(share):
    rows, depth = share.shape
    tp = lax.axis_size("tp")
    tiles = lax.all_to_all(share.reshape(tp, rows // tp, depth), "tp", 0, 0, tiled=True)
    return jnp.sum(tiles.astype(F32), axis=0)


def rows_of_all(normed):
    tp = lax.axis_size("tp")
    tiles = lax.all_to_all(
        jnp.broadcast_to(normed[None], (tp, *normed.shape)), "tp", 0, 0, tiled=True
    )
    return tiles.reshape(-1, normed.shape[1])


def body(tokens, w_gate, w_up, w_down, w_mix_in, w_mix_out, pool_w, pool_scale, norm_gains):
    tp_size, tp_at = lax.axis_size("tp"), lax.axis_index("tp")
    fs_at = lax.axis_index("fs")
    z, y = fs_at // NY, fs_at % NY
    own_rows = tokens.shape[0] // tp_size
    width = w_gate.shape[1]
    whole = width // 128 * 128

    groups = [[k * NY + j for j in range(NY)] for k in range(NZ)]
    first = jnp.concatenate(
        [w_gate[:, :whole], w_up[:, :whole], w_gate[:, whole:], w_up[:, whole:]], axis=1
    )
    second = jnp.concatenate([w_mix_in, w_mix_out.T, w_down.T], axis=1)
    second_width = second.shape[1]
    first = lax.all_gather(first, "fs", axis=0, tiled=True, axis_index_groups=groups)
    second = jnp.pad(second, ((0, 0), (0, 2 * width - second_width)))
    payload = jnp.concatenate([first, second], axis=0)
    got = {0: payload}
    for k in range(1, 9):
        got[-k] = shift(got[-k + 1], dz=1)
        if k < 8:
            got[k] = shift(got[k - 1], dz=-1)

    pieces = []
    for batch in BATCHES:
        own = jnp.concatenate([got[s][128:, :second_width] for s in batch], axis=0)
        pieces += [own, shift(own, dy=1), shift(own, dy=2), shift(own, dy=-1)]

    first_block = lax.rem(z + 8, NZ)
    stream = rolled(tokens, first_block)
    gains = rolled(norm_gains, first_block)
    payloads = [got[s] for s in OFFSETS]

    stream_own = lax.dynamic_slice_in_dim(stream, tp_at * own_rows, own_rows, 0).astype(F32)
    normed = rms_scale(stream.astype(F32), gains[0]).astype(BF)
    hidden = gated(normed, payloads, width)
    mix_w, down_w = assemble(y.astype(jnp.int32)[None], pieces, width)
    stream_own = stream_own + 0.5 * rms_scale(sum_at_owner(down(hidden, down_w)), gains[1])
    normed = rms_scale(stream_own, gains[2]).astype(BF)
    share = mixer(
        lax.rem(tp_at, 4).astype(jnp.int32)[None], rows_of_all(normed), mix_w, pool_w[0], pool_scale[None]
    )
    stream_own = stream_own + rms_scale(sum_at_owner(share), gains[3])
    normed = rms_scale(stream_own, gains[4]).astype(BF)
    hidden = gated(rows_of_all(normed), payloads, width)
    stream_own = stream_own + 0.5 * rms_scale(sum_at_owner(down(hidden, down_w)), gains[5])
    return rolled(stream_own.astype(BF), lax.rem(NZ + 8 - z, NZ))


def solution(mesh):
    in_specs = (
        P("fs", None),
        P("fs", "tp"),
        P("fs", "tp"),
        P("tp", "fs"),
        P("fs", "tp"),
        P("tp", "fs"),
        P("tp", None, None),
        P("tp"),
        P(),
    )
    out_specs = P(("fs", "tp"), None)
    return jax.shard_map(body, mesh=mesh, in_specs=in_specs, out_specs=out_specs, check_vma=False)
```

```python
import functools

import jax
import jax.numpy as jnp
from jax import lax
from jax.experimental import pallas as pl
from jax.experimental.pallas import tpu as pltpu
from jax.sharding import PartitionSpec as P


LEN = 64
NZ, NY = 16, 4
BF = jnp.bfloat16
F32 = jnp.float32
VMEM = pl.BlockSpec(memory_space=pltpu.VMEM)
SMEM = pl.BlockSpec(memory_space=pltpu.SMEM)


def limit(mib):
    return pltpu.CompilerParams(vmem_limit_bytes=mib * 1024 * 1024)


OFFSETS = tuple(range(-8, 8))
BATCHES = ((0, -1, 1, -2, 2, -3, 3, -4, 4, -5, 5), (-6, 6, -7, 7, -8))


def fs_shift(dy, dz):
    return [
        (z * NY + y, ((z + dz) % NZ) * NY + (y + dy) % NY) for z in range(NZ) for y in range(NY)
    ]


def shift(array, dy=0, dz=0):
    return lax.ppermute(array, "fs", fs_shift(dy, dz))


def rolled(array, first_block):
    twice = jnp.concatenate([array, array], axis=1)
    return lax.dynamic_slice_in_dim(twice, first_block * 128, array.shape[1], 1)


def pack_kernel(gate_ref, up_ref, in_ref, out_ref, down_ref, first_ref, second_ref):
    width = gate_ref.shape[1]
    whole = width // 128 * 128
    first_ref[:, :whole] = gate_ref[:, :whole]
    first_ref[:, whole : 2 * whole] = up_ref[:, :whole]
    first_ref[:, 2 * whole :] = jnp.concatenate([gate_ref[:, whole:], up_ref[:, whole:]], axis=1)
    second_ref[:, 0:128] = in_ref[...]
    second_ref[:, 128:256] = out_ref[...]
    second_ref[:, 256 : 256 + width] = down_ref[...]
    second_ref[:, 256 + width :] = jnp.zeros((32, width - 256), BF)


def pack(gate, up, mix_in, mix_out, down_w):
    shape = jax.ShapeDtypeStruct((32, 2 * gate.shape[1]), BF)
    return pl.pallas_call(
        pack_kernel,
        out_shape=(shape, shape),
        in_specs=[VMEM] * 5,
        out_specs=(VMEM, VMEM),
        compiler_params=limit(4),
        cost_estimate=pl.CostEstimate(flops=10**8, bytes_accessed=1 << 18, transcendentals=0),
        name="pack",
    )(gate, up, mix_in, mix_out, down_w)


def by_core(core, blocks):
    even, odd = blocks[0::2], blocks[1::2]
    mine = [jnp.where(core == 0, a, b) for a, b in zip(even, odd)]
    other = [jnp.where(core == 0, b, a) for a, b in zip(even, odd)]
    return jnp.concatenate(mine + other, axis=0)


def first_norm_kernel(at_ref, x_ref, gain_ref, out_ref):
    rows, depth = x_ref.shape
    tile = rows // 8
    block, core = at_ref[0], at_ref[1]
    halves = ([], [])
    for i in range(4):
        x0 = x_ref[2 * i * tile : (2 * i + 1) * tile, :].astype(F32)
        x1 = x_ref[(2 * i + 1) * tile : (2 * i + 2) * tile, :].astype(F32)
        for k, x in enumerate((x0, x1)):
            scale = lax.rsqrt(jnp.mean(x * x, axis=-1, keepdims=True) + 1e-06)
            halves[k].append(scale)
    for p in range(depth // 128):
        start = pl.multiple_of(lax.rem(block + p, depth // 128) * 128, 128)
        gain = gain_ref[0:1, p * 128 : (p + 1) * 128]
        mine, other = [], []
        for i in range(4):
            x0 = x_ref[2 * i * tile : (2 * i + 1) * tile, pl.ds(start, 128)].astype(F32)
            x1 = x_ref[(2 * i + 1) * tile : (2 * i + 2) * tile, pl.ds(start, 128)].astype(F32)
            x0 = (x0 * halves[0][i] * gain).astype(BF)
            x1 = (x1 * halves[1][i] * gain).astype(BF)
            mine.append(jnp.where(core == 0, x0, x1))
            other.append(jnp.where(core == 0, x1, x0))
        for i in range(4):
            out_ref[i * tile : (i + 1) * tile, p * 128 : (p + 1) * 128] = mine[i]
            out_ref[(4 + i) * tile : (5 + i) * tile, p * 128 : (p + 1) * 128] = other[i]


def first_norm(at, tokens, gain):
    return pl.pallas_call(
        first_norm_kernel,
        out_shape=jax.ShapeDtypeStruct(tokens.shape, BF),
        in_specs=[SMEM, VMEM, VMEM],
        out_specs=VMEM,
        compiler_params=limit(8),
        cost_estimate=pl.CostEstimate(flops=10**9, bytes_accessed=3 << 20, transcendentals=0),
        name="first_norm",
    )(at, tokens, gain)


def rms_scale(values, gain):
    return values * lax.rsqrt(jnp.mean(values * values, axis=-1, keepdims=True) + 1e-06) * gain


def settle_kernel(factor, parts_ref, stream_ref, gain_ref, next_ref, new_ref, normed_ref):
    total = parts_ref[0].astype(F32)
    for k in range(1, parts_ref.shape[0]):
        total = total + parts_ref[k].astype(F32)
    stream = stream_ref[...] + factor * rms_scale(total, gain_ref[...])
    new_ref[...] = stream
    normed_ref[...] = rms_scale(stream, next_ref[...]).astype(BF)


def settle(parts, stream, gain, next_gain, factor):
    return pl.pallas_call(
        functools.partial(settle_kernel, factor),
        out_shape=(
            jax.ShapeDtypeStruct(stream.shape, F32),
            jax.ShapeDtypeStruct(stream.shape, BF),
        ),
        in_specs=[VMEM] * 4,
        out_specs=(VMEM, VMEM),
        compiler_params=limit(6),
        cost_estimate=pl.CostEstimate(flops=10**8, bytes_accessed=1 << 20, transcendentals=0),
        name="settle",
    )(parts, stream, gain, next_gain)


def finish_kernel(at_ref, parts_ref, stream_ref, gain_ref, out_ref):
    total = parts_ref[0].astype(F32)
    for k in range(1, parts_ref.shape[0]):
        total = total + parts_ref[k].astype(F32)
    result = (stream_ref[...] + 0.5 * rms_scale(total, gain_ref[...])).astype(BF)
    blocks = result.shape[1] // 128
    for p in range(blocks):
        start = pl.multiple_of(lax.rem(at_ref[0] + p, blocks) * 128, 128)
        out_ref[:, pl.ds(start, 128)] = result[:, p * 128 : (p + 1) * 128]


def finish(at, parts, stream, gain):
    return pl.pallas_call(
        finish_kernel,
        out_shape=jax.ShapeDtypeStruct(stream.shape, BF),
        in_specs=[SMEM] + [VMEM] * 3,
        out_specs=VMEM,
        compiler_params=limit(6),
        cost_estimate=pl.CostEstimate(flops=10**8, bytes_accessed=1 << 20, transcendentals=0),
        name="finish",
    )(at, parts, stream, gain)


def gated_kernel(width, parts, *refs):
    payloads, out_ref, w_ref = refs[parts : parts + NZ], refs[-2], refs[-1]
    for k in range(NZ):
        w_ref[k * 128 : (k + 1) * 128, :] = payloads[k][0:128, :]
    x = jnp.concatenate([ref[...] for ref in refs[:parts]], axis=0)
    whole = width // 128 * 128

    def act(gate, up):
        return (gate / (1.0 + jnp.exp(-gate)) * up).astype(BF)

    at = 0
    while at < whole:
        n = min(256, whole - at)
        gate = jnp.dot(x, w_ref[:, at : at + n], preferred_element_type=F32)
        up = jnp.dot(x, w_ref[:, whole + at : whole + at + n], preferred_element_type=F32)
        out_ref[:, at : at + n] = act(gate, up)
        at += n
    if width > whole:
        rest = width - whole
        both = jnp.dot(x, w_ref[:, 2 * whole :], preferred_element_type=F32)
        out_ref[:, whole:] = act(both[:, :rest], both[:, rest:])


def gated(xs, payloads, width):
    rows, depth = sum(x.shape[0] for x in xs), xs[0].shape[1]
    return pl.pallas_call(
        functools.partial(gated_kernel, width, len(xs)),
        out_shape=jax.ShapeDtypeStruct((rows, width), BF),
        in_specs=[VMEM] * (len(xs) + NZ),
        out_specs=VMEM,
        scratch_shapes=[pltpu.VMEM((depth, 2 * width), BF)],
        compiler_params=limit(24),
        cost_estimate=pl.CostEstimate(
            flops=4 * rows * depth * width, bytes_accessed=8 << 20, transcendentals=0
        ),
        name="gated",
    )(*xs, *payloads)


def assemble_kernel(y_ref, *refs):
    ins, mix_ref, down_ref = refs[:-2], refs[-2], refs[-1]
    y = y_ref[0]
    at = 0
    for batch in BATCHES:
        for j in range(NY):
            src = ins[at]
            at += 1
            owner = lax.rem(y - j + NY, NY)
            for i, offset in enumerate(batch):
                start = pl.multiple_of(OFFSETS.index(offset) * 128 + owner * 32, 32)
                mix_ref[pl.ds(start, 32), :] = src[i * 32 : (i + 1) * 32, 0:256]
                down_ref[pl.ds(start, 32), :] = src[i * 32 : (i + 1) * 32, 256:]


def assemble(y, pieces, down_width):
    rows = NZ * NY * 32
    return pl.pallas_call(
        assemble_kernel,
        out_shape=(
            jax.ShapeDtypeStruct((rows, 256), BF),
            jax.ShapeDtypeStruct((rows, down_width), BF),
        ),
        in_specs=[SMEM] + [VMEM] * len(pieces),
        out_specs=(VMEM, VMEM),
        compiler_params=limit(14),
        cost_estimate=pl.CostEstimate(flops=10**8, bytes_accessed=8 << 20, transcendentals=0),
        name="assemble",
    )(y, *pieces)


def down_kernel(h_ref, w_ref, mine_ref, other_ref):
    h = h_ref[...]
    half = h.shape[0] // 2
    for at in range(0, w_ref.shape[0], 256):
        share = lax.dot_general(
            h, w_ref[at : at + 256, :], (((1,), (1,)), ((), ())), preferred_element_type=F32
        ).astype(BF)
        mine_ref[:, at : at + 256] = share[:half]
        other_ref[:, at : at + 256] = share[half:]


def down(hidden, w):
    rows, out = hidden.shape[0], w.shape[0]
    return pl.pallas_call(
        down_kernel,
        out_shape=(jax.ShapeDtypeStruct((rows // 2, out), BF),) * 2,
        in_specs=[VMEM, VMEM],
        out_specs=(VMEM, VMEM),
        compiler_params=limit(14),
        cost_estimate=pl.CostEstimate(
            flops=2 * rows * out * w.shape[1], bytes_accessed=4 << 20, transcendentals=0
        ),
        name="down",
    )(hidden, w)


def mixer_kernel(kind_ref, mine_ref, other_ref, w_ref, pool_ref, scale_ref, keep_ref, send_ref):
    rows = 2 * mine_ref.shape[0]
    tile = rows // 8
    kind, core = kind_ref[0], kind_ref[1]
    x = jnp.concatenate([mine_ref[...], other_ref[...]], axis=0)
    values = jnp.dot(x, w_ref[:, 0:128], preferred_element_type=F32)
    values = values.astype(BF).astype(F32)
    in_order = []
    for i in range(4):
        mine = values[i * tile : (i + 1) * tile]
        other = values[(4 + i) * tile : (5 + i) * tile]
        in_order += [jnp.where(core == 0, mine, other), jnp.where(core == 0, other, mine)]
    values = jnp.concatenate(in_order, axis=0)
    place = lax.broadcasted_iota(jnp.int32, (rows, 128), 0) % LEN
    total = values
    chosen = jnp.zeros_like(values)
    for slot in range(4):
        lag = 2**slot
        earlier = jnp.concatenate([jnp.zeros((lag, 128), F32), total[: rows - lag]], axis=0)
        total = total + jnp.where(place >= lag, earlier, 0.0)
        window = 2 * lag
        mean = total / jnp.minimum(place + 1, window).astype(F32)
        chosen = jnp.where(kind == slot, mean, chosen)
    deviation = (chosen - values).astype(BF)
    mixed = jnp.dot(deviation, pool_ref[...], preferred_element_type=F32)
    mixed = mixed * scale_ref[...].astype(F32)
    mixed = by_core(core, [mixed[i * tile : (i + 1) * tile] for i in range(8)]).astype(BF)
    for at in range(0, w_ref.shape[0], 256):
        share = lax.dot_general(
            mixed, w_ref[at : at + 256, 128:256], (((1,), (1,)), ((), ())), preferred_element_type=F32
        ).astype(BF)
        keep_ref[:, at : at + 256] = share[: rows // 2]
        send_ref[:, at : at + 256] = share[rows // 2 :]


def mixer(kind, mine, other, w, pool_w, pool_scale):
    rows, depth = 2 * mine.shape[0], mine.shape[1]
    return pl.pallas_call(
        mixer_kernel,
        out_shape=(jax.ShapeDtypeStruct((rows // 2, depth), BF),) * 2,
        in_specs=[SMEM] + [VMEM] * 5,
        out_specs=(VMEM, VMEM),
        compiler_params=limit(14),
        cost_estimate=pl.CostEstimate(
            flops=4 * rows * depth * 128, bytes_accessed=4 << 20, transcendentals=0
        ),
        name="mixer",
    )(kind, mine, other, w, pool_w, pool_scale)


X_GROUPS = [[2 * x + core for x in range(4)] for core in range(2)]


def core_swap(array):
    return lax.ppermute(array, "tp", [(k, k ^ 1) for k in range(8)])


def shares_of_rows(mine, other):
    both = (mine.astype(F32) + core_swap(other).astype(F32)).astype(BF)
    tiles = both.reshape(4, both.shape[0] // 4, both.shape[1])
    return lax.all_to_all(tiles, "tp", 0, 0, tiled=True, axis_index_groups=X_GROUPS)


def rows_of_all(normed):
    mine = lax.all_gather(normed, "tp", axis=0, tiled=True, axis_index_groups=X_GROUPS)
    return mine, core_swap(mine)


def body(tokens, w_gate, w_up, w_down, w_mix_in, w_mix_out, pool_w, pool_scale, norm_gains):
    tp_size, tp_at = lax.axis_size("tp"), lax.axis_index("tp")
    fs_at = lax.axis_index("fs")
    z, y = fs_at // NY, fs_at % NY
    own_rows = tokens.shape[0] // tp_size
    width = w_gate.shape[1]
    whole = width // 128 * 128

    groups = [[k * NY + j for j in range(NY)] for k in range(NZ)]
    first, second = pack(w_gate, w_up, w_mix_in, w_mix_out.T, w_down.T)
    second_width = 256 + width
    first = lax.all_gather(first, "fs", axis=0, tiled=True, axis_index_groups=groups)
    payload = jnp.concatenate([first, second], axis=0)
    got = {0: payload}
    for k in range(1, 9):
        got[-k] = shift(got[-k + 1], dz=1)
        if k < 8:
            got[k] = shift(got[k - 1], dz=-1)

    pieces = []
    for batch in BATCHES:
        own = jnp.concatenate([got[s][128:, :second_width] for s in batch], axis=0)
        pieces += [own, shift(own, dy=1), shift(own, dy=2), shift(own, dy=-1)]

    first_block = lax.rem(z + 8, NZ)
    core = lax.rem(tp_at, 2)
    gains = rolled(norm_gains, first_block)
    gain = [gains[k : k + 1] for k in range(6)]
    payloads = [got[s] for s in OFFSETS]
    numbers = jnp.stack([first_block, core, lax.rem(tp_at, 4), y]).astype(jnp.int32)

    stream = lax.dynamic_slice_in_dim(tokens, tp_at * own_rows, own_rows, 0)
    stream = rolled(stream, first_block).astype(F32)
    hidden = gated([first_norm(numbers[0:2], tokens, gain[0])], payloads, width)
    mix_w, down_w = assemble(numbers[3:4], pieces, width)
    parts = shares_of_rows(*down(hidden, down_w))
    stream, normed = settle(parts, stream, gain[1], gain[2], 0.5)
    kind = jnp.stack([numbers[2], numbers[1]])
    share = mixer(kind, *rows_of_all(normed), mix_w, pool_w[0], pool_scale[None])
    stream, normed = settle(shares_of_rows(*share), stream, gain[3], gain[4], 1.0)
    hidden = gated(rows_of_all(normed), payloads, width)
    parts = shares_of_rows(*down(hidden, down_w))
    return finish(numbers[0:1], parts, stream, gain[5])


def solution(mesh):
    in_specs = (
        P("fs", None),
        P("fs", "tp"),
        P("fs", "tp"),
        P("tp", "fs"),
        P("fs", "tp"),
        P("tp", "fs"),
        P("tp", None, None),
        P("tp"),
        P(),
    )
    out_specs = P(("fs", "tp"), None)
    return jax.shard_map(body, mesh=mesh, in_specs=in_specs, out_specs=out_specs, check_vma=False)
```

```python
import functools

import jax
import jax.numpy as jnp
from jax import lax
from jax.experimental import pallas as pl
from jax.experimental.pallas import tpu as pltpu
from jax.sharding import PartitionSpec as P


LEN = 64
NZ, NY = 16, 4
BF = jnp.bfloat16
F32 = jnp.float32
VMEM = pl.BlockSpec(memory_space=pltpu.VMEM)
SMEM = pl.BlockSpec(memory_space=pltpu.SMEM)


def limit(mib):
    return pltpu.CompilerParams(vmem_limit_bytes=mib * 1024 * 1024)


OFFSETS = tuple(range(-8, 8))
BATCHES = ((0, -1, 1, -2, 2, -3, 3, -4, 4, -5, 5), (-6, 6, -7, 7, -8))
HBM = pl.BlockSpec(memory_space=pltpu.HBM)


def fs_shift(dy, dz):
    return [
        (z * NY + y, ((z + dz) % NZ) * NY + (y + dy) % NY) for z in range(NZ) for y in range(NY)
    ]


def shift(array, dy=0, dz=0):
    return lax.ppermute(array, "fs", fs_shift(dy, dz))


def rolled(array, first_block):
    twice = jnp.concatenate([array, array], axis=1)
    return lax.dynamic_slice_in_dim(twice, first_block * 128, array.shape[1], 1)


def pack_kernel(gate_in, up_in, mix_in, mix_out, down_in, first_ref, second_ref, *scratch):
    held, sems = scratch[:5], scratch[5]
    copies = []
    for k, (src, dst) in enumerate(zip((gate_in, up_in, mix_in, mix_out, down_in), held)):
        copies.append(pltpu.make_async_copy(src, dst, sems.at[k]))
        copies[-1].start()
    for copy in copies:
        copy.wait()
    gate_ref, up_ref, in_ref, out_ref, down_ref = held
    width = gate_ref.shape[1]
    whole = width // 128 * 128
    first_ref[:, :whole] = gate_ref[:, :whole]
    first_ref[:, whole : 2 * whole] = up_ref[:, :whole]
    first_ref[:, 2 * whole :] = jnp.concatenate([gate_ref[:, whole:], up_ref[:, whole:]], axis=1)
    second_ref[:, 0:128] = in_ref[...]
    second_ref[:, 128:256] = out_ref[...]
    second_ref[:, 256 : 256 + width] = down_ref[...]
    second_ref[:, 256 + width :] = jnp.zeros((32, width - 256), BF)


def pack(*weights):
    shape = jax.ShapeDtypeStruct((32, 2 * weights[0].shape[1]), BF)
    return pl.pallas_call(
        pack_kernel,
        out_shape=(shape, shape),
        in_specs=[HBM] * 5,
        out_specs=(VMEM, VMEM),
        scratch_shapes=[pltpu.VMEM(w.shape, BF) for w in weights] + [pltpu.SemaphoreType.DMA((5,))],
        compiler_params=limit(63),
        cost_estimate=pl.CostEstimate(flops=10**8, bytes_accessed=1 << 18, transcendentals=0),
        name="pack",
    )(*weights)


def join_kernel(first_ref, back_ref, ahead_ref, to_next_ref, to_last_ref):
    rows = first_ref.shape[0]
    for ref, second in ((to_next_ref, back_ref), (to_last_ref, ahead_ref)):
        ref[:rows, :] = first_ref[...]
        ref[rows:, :] = second[...]


def join(first, back, ahead):
    shape = jax.ShapeDtypeStruct((first.shape[0] + back.shape[0], first.shape[1]), BF)
    return pl.pallas_call(
        join_kernel,
        out_shape=(shape, shape),
        in_specs=[VMEM] * 3,
        out_specs=(VMEM, VMEM),
        compiler_params=limit(6),
        cost_estimate=pl.CostEstimate(flops=10**8, bytes_accessed=1 << 18, transcendentals=0),
        name="join",
    )(first, back, ahead)


def by_core(core, blocks):
    even, odd = blocks[0::2], blocks[1::2]
    mine = [jnp.where(core == 0, a, b) for a, b in zip(even, odd)]
    other = [jnp.where(core == 0, b, a) for a, b in zip(even, odd)]
    return jnp.concatenate(mine + other, axis=0)


def first_norm_kernel(at_ref, x_ref, gain_ref, out_ref):
    rows, depth = x_ref.shape
    tile = rows // 8
    block, core = at_ref[0], at_ref[1]
    halves = ([], [])
    for i in range(4):
        x0 = x_ref[2 * i * tile : (2 * i + 1) * tile, :].astype(F32)
        x1 = x_ref[(2 * i + 1) * tile : (2 * i + 2) * tile, :].astype(F32)
        for k, x in enumerate((x0, x1)):
            scale = lax.rsqrt(jnp.mean(x * x, axis=-1, keepdims=True) + 1e-06)
            halves[k].append(scale)
    for p in range(depth // 128):
        start = pl.multiple_of(lax.rem(block + p, depth // 128) * 128, 128)
        gain = gain_ref[0:1, p * 128 : (p + 1) * 128]
        mine, other = [], []
        for i in range(4):
            x0 = x_ref[2 * i * tile : (2 * i + 1) * tile, pl.ds(start, 128)].astype(F32)
            x1 = x_ref[(2 * i + 1) * tile : (2 * i + 2) * tile, pl.ds(start, 128)].astype(F32)
            x0 = (x0 * halves[0][i] * gain).astype(BF)
            x1 = (x1 * halves[1][i] * gain).astype(BF)
            mine.append(jnp.where(core == 0, x0, x1))
            other.append(jnp.where(core == 0, x1, x0))
        for i in range(4):
            out_ref[i * tile : (i + 1) * tile, p * 128 : (p + 1) * 128] = mine[i]
            out_ref[(4 + i) * tile : (5 + i) * tile, p * 128 : (p + 1) * 128] = other[i]


def first_norm(at, tokens, gain):
    return pl.pallas_call(
        first_norm_kernel,
        out_shape=jax.ShapeDtypeStruct(tokens.shape, BF),
        in_specs=[SMEM, VMEM, VMEM],
        out_specs=VMEM,
        compiler_params=limit(8),
        cost_estimate=pl.CostEstimate(flops=10**9, bytes_accessed=3 << 20, transcendentals=0),
        name="first_norm",
    )(at, tokens, gain)


def rms_scale(values, gain):
    return values * lax.rsqrt(jnp.mean(values * values, axis=-1, keepdims=True) + 1e-06) * gain


def settle_kernel(factor, parts_ref, stream_ref, gain_ref, next_ref, new_ref, normed_ref):
    total = parts_ref[0].astype(F32)
    for k in range(1, parts_ref.shape[0]):
        total = total + parts_ref[k].astype(F32)
    stream = stream_ref[...] + factor * rms_scale(total, gain_ref[...])
    new_ref[...] = stream
    normed_ref[...] = rms_scale(stream, next_ref[...]).astype(BF)


def settle(parts, stream, gain, next_gain, factor):
    return pl.pallas_call(
        functools.partial(settle_kernel, factor),
        out_shape=(
            jax.ShapeDtypeStruct(stream.shape, F32),
            jax.ShapeDtypeStruct(stream.shape, BF),
        ),
        in_specs=[VMEM] * 4,
        out_specs=(VMEM, VMEM),
        compiler_params=limit(6),
        cost_estimate=pl.CostEstimate(flops=10**8, bytes_accessed=1 << 20, transcendentals=0),
        name="settle",
    )(parts, stream, gain, next_gain)


def finish_kernel(at_ref, parts_ref, stream_ref, gain_ref, out_ref):
    total = parts_ref[0].astype(F32)
    for k in range(1, parts_ref.shape[0]):
        total = total + parts_ref[k].astype(F32)
    result = (stream_ref[...] + 0.5 * rms_scale(total, gain_ref[...])).astype(BF)
    blocks = result.shape[1] // 128
    for p in range(blocks):
        start = pl.multiple_of(lax.rem(at_ref[0] + p, blocks) * 128, 128)
        out_ref[:, pl.ds(start, 128)] = result[:, p * 128 : (p + 1) * 128]


def finish(at, parts, stream, gain):
    return pl.pallas_call(
        finish_kernel,
        out_shape=jax.ShapeDtypeStruct(stream.shape, BF),
        in_specs=[SMEM] + [VMEM] * 3,
        out_specs=VMEM,
        compiler_params=limit(6),
        cost_estimate=pl.CostEstimate(flops=10**8, bytes_accessed=1 << 20, transcendentals=0),
        name="finish",
    )(at, parts, stream, gain)


def gated_kernel(width, parts, *refs):
    payloads, out_ref, w_ref = refs[parts : parts + NZ], refs[-2], refs[-1]
    for k in range(NZ):
        w_ref[k * 128 : (k + 1) * 128, :] = payloads[k][0:128, :]
    x = jnp.concatenate([ref[...] for ref in refs[:parts]], axis=0)
    whole = width // 128 * 128

    def act(gate, up):
        return (gate / (1.0 + jnp.exp(-gate)) * up).astype(BF)

    at = 0
    while at < whole:
        n = min(256, whole - at)
        gate = jnp.dot(x, w_ref[:, at : at + n], preferred_element_type=F32)
        up = jnp.dot(x, w_ref[:, whole + at : whole + at + n], preferred_element_type=F32)
        out_ref[:, at : at + n] = act(gate, up)
        at += n
    if width > whole:
        rest = width - whole
        both = jnp.dot(x, w_ref[:, 2 * whole :], preferred_element_type=F32)
        out_ref[:, whole:] = act(both[:, :rest], both[:, rest:])


def gated(xs, payloads, width):
    rows, depth = sum(x.shape[0] for x in xs), xs[0].shape[1]
    return pl.pallas_call(
        functools.partial(gated_kernel, width, len(xs)),
        out_shape=jax.ShapeDtypeStruct((rows, width), BF),
        in_specs=[VMEM] * (len(xs) + NZ),
        out_specs=VMEM,
        scratch_shapes=[pltpu.VMEM((depth, 2 * width), BF)],
        compiler_params=limit(24),
        cost_estimate=pl.CostEstimate(
            flops=4 * rows * depth * width, bytes_accessed=8 << 20, transcendentals=0
        ),
        name="gated",
    )(*xs, *payloads)


def assemble_kernel(batch, y_ref, *refs):
    ins, mix_ref, down_ref = refs[:NY], refs[-2], refs[-1]
    y = y_ref[0]
    width = mix_ref.shape[1] + down_ref.shape[1]
    for j in range(NY):
        owner = lax.rem(y - j + NY, NY)
        for i, offset in enumerate(batch):
            start = pl.multiple_of(OFFSETS.index(offset) * 128 + owner * 32, 32)
            mix_ref[pl.ds(start, 32), :] = ins[j][i * 32 : (i + 1) * 32, 0:256]
            down_ref[pl.ds(start, 32), :] = ins[j][i * 32 : (i + 1) * 32, 256:width]


def assemble(y, pieces, batch, down_width, before=()):
    rows = NZ * NY * 32
    return pl.pallas_call(
        functools.partial(assemble_kernel, batch),
        out_shape=(
            jax.ShapeDtypeStruct((rows, 256), BF),
            jax.ShapeDtypeStruct((rows, down_width), BF),
        ),
        in_specs=[SMEM] + [VMEM] * (NY + len(before)),
        out_specs=(VMEM, VMEM),
        input_output_aliases={1 + NY: 0, 2 + NY: 1} if before else {},
        compiler_params=limit(12),
        cost_estimate=pl.CostEstimate(flops=10**8, bytes_accessed=8 << 20, transcendentals=0),
        name="assemble",
    )(y, *pieces, *before)


def down_kernel(h_ref, w_ref, mine_ref, other_ref):
    h = h_ref[...]
    half = h.shape[0] // 2
    for at in range(0, w_ref.shape[0], 256):
        share = lax.dot_general(
            h, w_ref[at : at + 256, :], (((1,), (1,)), ((), ())), preferred_element_type=F32
        ).astype(BF)
        mine_ref[:, at : at + 256] = share[:half]
        other_ref[:, at : at + 256] = share[half:]


def down(hidden, w):
    rows, out = hidden.shape[0], w.shape[0]
    return pl.pallas_call(
        down_kernel,
        out_shape=(jax.ShapeDtypeStruct((rows // 2, out), BF),) * 2,
        in_specs=[VMEM, VMEM],
        out_specs=(VMEM, VMEM),
        compiler_params=limit(14),
        cost_estimate=pl.CostEstimate(
            flops=2 * rows * out * w.shape[1], bytes_accessed=4 << 20, transcendentals=0
        ),
        name="down",
    )(hidden, w)


def mixer_kernel(kind_ref, mine_ref, other_ref, w_ref, pool_ref, scale_ref, keep_ref, send_ref):
    rows = 2 * mine_ref.shape[0]
    tile = rows // 8
    kind, core = kind_ref[0], kind_ref[1]
    x = jnp.concatenate([mine_ref[...], other_ref[...]], axis=0)
    values = jnp.dot(x, w_ref[:, 0:128], preferred_element_type=F32)
    values = values.astype(BF).astype(F32)
    in_order = []
    for i in range(4):
        mine = values[i * tile : (i + 1) * tile]
        other = values[(4 + i) * tile : (5 + i) * tile]
        in_order += [jnp.where(core == 0, mine, other), jnp.where(core == 0, other, mine)]
    values = jnp.concatenate(in_order, axis=0)
    place = lax.broadcasted_iota(jnp.int32, (rows, 128), 0) % LEN
    total = values
    chosen = jnp.zeros_like(values)
    for slot in range(4):
        lag = 2**slot
        earlier = jnp.concatenate([jnp.zeros((lag, 128), F32), total[: rows - lag]], axis=0)
        total = total + jnp.where(place >= lag, earlier, 0.0)
        window = 2 * lag
        mean = total / jnp.minimum(place + 1, window).astype(F32)
        chosen = jnp.where(kind == slot, mean, chosen)
    deviation = (chosen - values).astype(BF)
    mixed = jnp.dot(deviation, pool_ref[...], preferred_element_type=F32)
    mixed = mixed * scale_ref[...].astype(F32)
    mixed = by_core(core, [mixed[i * tile : (i + 1) * tile] for i in range(8)]).astype(BF)
    for at in range(0, w_ref.shape[0], 256):
        share = lax.dot_general(
            mixed, w_ref[at : at + 256, 128:256], (((1,), (1,)), ((), ())), preferred_element_type=F32
        ).astype(BF)
        keep_ref[:, at : at + 256] = share[: rows // 2]
        send_ref[:, at : at + 256] = share[rows // 2 :]


def mixer(kind, mine, other, w, pool_w, pool_scale):
    rows, depth = 2 * mine.shape[0], mine.shape[1]
    return pl.pallas_call(
        mixer_kernel,
        out_shape=(jax.ShapeDtypeStruct((rows // 2, depth), BF),) * 2,
        in_specs=[SMEM] + [VMEM] * 5,
        out_specs=(VMEM, VMEM),
        compiler_params=limit(14),
        cost_estimate=pl.CostEstimate(
            flops=4 * rows * depth * 128, bytes_accessed=4 << 20, transcendentals=0
        ),
        name="mixer",
    )(kind, mine, other, w, pool_w, pool_scale)


X_GROUPS = [[2 * x + core for x in range(4)] for core in range(2)]


def core_swap(array):
    return lax.ppermute(array, "tp", [(k, k ^ 1) for k in range(8)])


def shares_of_rows(mine, other):
    both = (mine.astype(F32) + core_swap(other).astype(F32)).astype(BF)
    tiles = both.reshape(4, both.shape[0] // 4, both.shape[1])
    return lax.all_to_all(tiles, "tp", 0, 0, tiled=True, axis_index_groups=X_GROUPS)


def rows_of_all(normed):
    mine = lax.all_gather(normed, "tp", axis=0, tiled=True, axis_index_groups=X_GROUPS)
    return mine, core_swap(mine)


def body(tokens, w_gate, w_up, w_down, w_mix_in, w_mix_out, pool_w, pool_scale, norm_gains):
    tp_size, tp_at = lax.axis_size("tp"), lax.axis_index("tp")
    fs_at = lax.axis_index("fs")
    z, y = fs_at // NY, fs_at % NY
    own_rows = tokens.shape[0] // tp_size
    width = w_gate.shape[1]
    whole = width // 128 * 128

    groups = [[k * NY + j for j in range(NY)] for k in range(NZ)]
    first, second = pack(w_gate, w_up, w_mix_in, w_mix_out.T, w_down.T)
    seconds = {0: second, -1: shift(second, dz=1), 1: shift(second, dz=-1)}
    first = lax.all_gather(first, "fs", axis=0, tiled=True, axis_index_groups=groups)
    back, ahead = join(first, seconds[-1], seconds[1])

    first_block = lax.rem(z + 8, NZ)
    core = lax.rem(tp_at, 2)
    gains = rolled(norm_gains, first_block)
    gain = [gains[k : k + 1] for k in range(6)]
    numbers = jnp.stack([first_block, core, lax.rem(tp_at, 4), y]).astype(jnp.int32)
    got = {0: back}
    for k in range(1, 9):
        back = got[-k] = shift(back if k < 8 else back[:128], dz=1)
        if k < 8:
            ahead = got[k] = shift(ahead, dz=-1)
            seconds[-k - 1] = back[128:]
            seconds[k + 1] = ahead[128:]
        if k == 2:
            back, ahead, late_tokens = lax.optimization_barrier((back, ahead, tokens))
            x = first_norm(numbers[0:2], late_tokens, gain[0])
        if k == 5:
            back, ahead, x = lax.optimization_barrier((back, ahead, x))
        if k < 8:
            got[-k], got[k] = back, ahead
    payloads = [got[k] for k in OFFSETS]

    late = ()
    for batch in BATCHES:
        own = jnp.concatenate([seconds[s][:, : 256 + width] for s in batch], axis=0)
        pieces = [own, shift(own, dy=1), shift(own, dy=2), shift(own, dy=-1)]
        late = assemble(numbers[3:4], pieces, batch, width, late)
    mix_w, down_w = late

    stream = lax.dynamic_slice_in_dim(tokens, tp_at * own_rows, own_rows, 0)
    stream = rolled(stream, first_block).astype(F32)
    parts = shares_of_rows(*down(gated([x], payloads, width), down_w))
    stream, normed = settle(parts, stream, gain[1], gain[2], 0.5)
    kind = jnp.stack([numbers[2], numbers[1]])
    share = mixer(kind, *rows_of_all(normed), mix_w, pool_w[0], pool_scale[None])
    stream, normed = settle(shares_of_rows(*share), stream, gain[3], gain[4], 1.0)
    hidden = gated(rows_of_all(normed), payloads, width)
    parts = shares_of_rows(*down(hidden, down_w))
    return finish(numbers[0:1], parts, stream, gain[5])


def solution(mesh):
    in_specs = (
        P("fs", None),
        P("fs", "tp"),
        P("fs", "tp"),
        P("tp", "fs"),
        P("fs", "tp"),
        P("tp", "fs"),
        P("tp", None, None),
        P("tp"),
        P(),
    )
    out_specs = P(("fs", "tp"), None)
    return jax.shard_map(body, mesh=mesh, in_specs=in_specs, out_specs=out_specs, check_vma=False)
```

```python
import functools

import jax
import jax.numpy as jnp
from jax import lax
from jax.experimental import pallas as pl
from jax.experimental.pallas import tpu as pltpu
from jax.sharding import PartitionSpec as P


LEN = 64
NZ, NY = 16, 4
BF = jnp.bfloat16
F32 = jnp.float32
VMEM = pl.BlockSpec(memory_space=pltpu.VMEM)
SMEM = pl.BlockSpec(memory_space=pltpu.SMEM)


def limit(mib):
    return pltpu.CompilerParams(vmem_limit_bytes=mib * 1024 * 1024)


OFFSETS = tuple(range(-8, 8))
BATCHES = ((0, -1, 1, -2, 2, -3, 3, -4, 4, -5, 5), (-6, 6, -7, 7, -8))
HBM = pl.BlockSpec(memory_space=pltpu.HBM)


def fs_shift(dy, dz):
    return [
        (z * NY + y, ((z + dz) % NZ) * NY + (y + dy) % NY) for z in range(NZ) for y in range(NY)
    ]


def shift(array, dy=0, dz=0):
    return lax.ppermute(array, "fs", fs_shift(dy, dz))


def rolled(array, first_block):
    twice = jnp.concatenate([array, array], axis=1)
    return lax.dynamic_slice_in_dim(twice, first_block * 128, array.shape[1], 1)


def pack_kernel(gate_in, up_in, mix_in, mix_out, down_in, first_ref, second_ref, *scratch):
    held, sems = scratch[:5], scratch[5]
    copies = []
    for k, (src, dst) in enumerate(zip((gate_in, up_in, mix_in, mix_out, down_in), held)):
        copies.append(pltpu.make_async_copy(src, dst, sems.at[k]))
        copies[-1].start()
    for copy in copies:
        copy.wait()
    gate_ref, up_ref, in_ref, out_ref, down_ref = held
    width = gate_ref.shape[1]
    whole = width // 128 * 128
    first_ref[:, :whole] = gate_ref[:, :whole]
    first_ref[:, whole : 2 * whole] = up_ref[:, :whole]
    first_ref[:, 2 * whole :] = jnp.concatenate([gate_ref[:, whole:], up_ref[:, whole:]], axis=1)
    second_ref[:, 0:128] = in_ref[...]
    second_ref[:, 128:256] = out_ref[...]
    second_ref[:, 256 : 256 + width] = down_ref[...]
    second_ref[:, 256 + width :] = jnp.zeros((32, width - 256), BF)


def pack(*weights):
    shape = jax.ShapeDtypeStruct((32, 2 * weights[0].shape[1]), BF)
    return pl.pallas_call(
        pack_kernel,
        out_shape=(shape, shape),
        in_specs=[HBM] * 5,
        out_specs=(VMEM, VMEM),
        scratch_shapes=[pltpu.VMEM(w.shape, BF) for w in weights] + [pltpu.SemaphoreType.DMA((5,))],
        compiler_params=limit(63),
        cost_estimate=pl.CostEstimate(flops=10**8, bytes_accessed=1 << 18, transcendentals=0),
        name="pack",
    )(*weights)


def by_core(core, blocks):
    even, odd = blocks[0::2], blocks[1::2]
    mine = [jnp.where(core == 0, a, b) for a, b in zip(even, odd)]
    other = [jnp.where(core == 0, b, a) for a, b in zip(even, odd)]
    return jnp.concatenate(mine + other, axis=0)


def first_norm_kernel(at_ref, x_ref, gain_ref, out_ref):
    rows, depth = x_ref.shape
    tile = rows // 8
    block, core = at_ref[0], at_ref[1]
    halves = ([], [])
    for i in range(4):
        x0 = x_ref[2 * i * tile : (2 * i + 1) * tile, :].astype(F32)
        x1 = x_ref[(2 * i + 1) * tile : (2 * i + 2) * tile, :].astype(F32)
        for k, x in enumerate((x0, x1)):
            scale = lax.rsqrt(jnp.mean(x * x, axis=-1, keepdims=True) + 1e-06)
            halves[k].append(scale)
    for p in range(depth // 128):
        start = pl.multiple_of(lax.rem(block + p, depth // 128) * 128, 128)
        gain = gain_ref[0:1, p * 128 : (p + 1) * 128]
        mine, other = [], []
        for i in range(4):
            x0 = x_ref[2 * i * tile : (2 * i + 1) * tile, pl.ds(start, 128)].astype(F32)
            x1 = x_ref[(2 * i + 1) * tile : (2 * i + 2) * tile, pl.ds(start, 128)].astype(F32)
            x0 = (x0 * halves[0][i] * gain).astype(BF)
            x1 = (x1 * halves[1][i] * gain).astype(BF)
            mine.append(jnp.where(core == 0, x0, x1))
            other.append(jnp.where(core == 0, x1, x0))
        for i in range(4):
            out_ref[i * tile : (i + 1) * tile, p * 128 : (p + 1) * 128] = mine[i]
            out_ref[(4 + i) * tile : (5 + i) * tile, p * 128 : (p + 1) * 128] = other[i]


def first_norm(at, tokens, gain):
    return pl.pallas_call(
        first_norm_kernel,
        out_shape=jax.ShapeDtypeStruct(tokens.shape, BF),
        in_specs=[SMEM, VMEM, VMEM],
        out_specs=VMEM,
        compiler_params=limit(8),
        cost_estimate=pl.CostEstimate(flops=10**9, bytes_accessed=3 << 20, transcendentals=0),
        name="first_norm",
    )(at, tokens, gain)


def rms_scale(values, gain):
    return values * lax.rsqrt(jnp.mean(values * values, axis=-1, keepdims=True) + 1e-06) * gain


def settle_kernel(factor, parts_ref, stream_ref, gain_ref, next_ref, new_ref, normed_ref):
    total = parts_ref[0].astype(F32)
    for k in range(1, parts_ref.shape[0]):
        total = total + parts_ref[k].astype(F32)
    stream = stream_ref[...] + factor * rms_scale(total, gain_ref[...])
    new_ref[...] = stream
    normed_ref[...] = rms_scale(stream, next_ref[...]).astype(BF)


def settle(parts, stream, gain, next_gain, factor):
    return pl.pallas_call(
        functools.partial(settle_kernel, factor),
        out_shape=(
            jax.ShapeDtypeStruct(stream.shape, F32),
            jax.ShapeDtypeStruct(stream.shape, BF),
        ),
        in_specs=[VMEM] * 4,
        out_specs=(VMEM, VMEM),
        compiler_params=limit(6),
        cost_estimate=pl.CostEstimate(flops=10**8, bytes_accessed=1 << 20, transcendentals=0),
        name="settle",
    )(parts, stream, gain, next_gain)


def finish_kernel(at_ref, parts_ref, stream_ref, gain_ref, out_ref):
    total = parts_ref[0].astype(F32)
    for k in range(1, parts_ref.shape[0]):
        total = total + parts_ref[k].astype(F32)
    result = (stream_ref[...] + 0.5 * rms_scale(total, gain_ref[...])).astype(BF)
    blocks = result.shape[1] // 128
    for p in range(blocks):
        start = pl.multiple_of(lax.rem(at_ref[0] + p, blocks) * 128, 128)
        out_ref[:, pl.ds(start, 128)] = result[:, p * 128 : (p + 1) * 128]


def finish(at, parts, stream, gain):
    return pl.pallas_call(
        finish_kernel,
        out_shape=jax.ShapeDtypeStruct(stream.shape, BF),
        in_specs=[SMEM] + [VMEM] * 3,
        out_specs=VMEM,
        compiler_params=limit(6),
        cost_estimate=pl.CostEstimate(flops=10**8, bytes_accessed=1 << 20, transcendentals=0),
        name="finish",
    )(at, parts, stream, gain)


def gated_kernel(width, parts, *refs):
    payloads, out_ref, w_ref = refs[parts : parts + NZ], refs[-2], refs[-1]
    for k in range(NZ):
        w_ref[k * 128 : (k + 1) * 128, :] = payloads[k][0:128, :]
    x = jnp.concatenate([ref[...] for ref in refs[:parts]], axis=0)
    whole = width // 128 * 128

    def act(gate, up):
        return (gate / (1.0 + jnp.exp(-gate)) * up).astype(BF)

    at = 0
    while at < whole:
        n = min(256, whole - at)
        gate = jnp.dot(x, w_ref[:, at : at + n], preferred_element_type=F32)
        up = jnp.dot(x, w_ref[:, whole + at : whole + at + n], preferred_element_type=F32)
        out_ref[:, at : at + n] = act(gate, up)
        at += n
    if width > whole:
        rest = width - whole
        both = jnp.dot(x, w_ref[:, 2 * whole :], preferred_element_type=F32)
        out_ref[:, whole:] = act(both[:, :rest], both[:, rest:])


def gated(xs, payloads, width):
    rows, depth = sum(x.shape[0] for x in xs), xs[0].shape[1]
    return pl.pallas_call(
        functools.partial(gated_kernel, width, len(xs)),
        out_shape=jax.ShapeDtypeStruct((rows, width), BF),
        in_specs=[VMEM] * (len(xs) + NZ),
        out_specs=VMEM,
        scratch_shapes=[pltpu.VMEM((depth, 2 * width), BF)],
        compiler_params=limit(24),
        cost_estimate=pl.CostEstimate(
            flops=4 * rows * depth * width, bytes_accessed=8 << 20, transcendentals=0
        ),
        name="gated",
    )(*xs, *payloads)


def assemble_kernel(batch, y_ref, *refs):
    ins, mix_ref, down_ref = refs[:NY], refs[-2], refs[-1]
    y = y_ref[0]
    width = mix_ref.shape[1] + down_ref.shape[1]
    for j in range(NY):
        owner = lax.rem(y - j + NY, NY)
        for i, offset in enumerate(batch):
            start = pl.multiple_of(OFFSETS.index(offset) * 128 + owner * 32, 32)
            mix_ref[pl.ds(start, 32), :] = ins[j][i * 32 : (i + 1) * 32, 0:256]
            down_ref[pl.ds(start, 32), :] = ins[j][i * 32 : (i + 1) * 32, 256:width]


def assemble(y, pieces, batch, down_width, before=()):
    rows = NZ * NY * 32
    return pl.pallas_call(
        functools.partial(assemble_kernel, batch),
        out_shape=(
            jax.ShapeDtypeStruct((rows, 256), BF),
            jax.ShapeDtypeStruct((rows, down_width), BF),
        ),
        in_specs=[SMEM] + [VMEM] * (NY + len(before)),
        out_specs=(VMEM, VMEM),
        input_output_aliases={1 + NY: 0, 2 + NY: 1} if before else {},
        compiler_params=limit(12),
        cost_estimate=pl.CostEstimate(flops=10**8, bytes_accessed=8 << 20, transcendentals=0),
        name="assemble",
    )(y, *pieces, *before)


def down_kernel(h_ref, w_ref, mine_ref, other_ref):
    h = h_ref[...]
    half = h.shape[0] // 2
    for at in range(0, w_ref.shape[0], 256):
        share = lax.dot_general(
            h, w_ref[at : at + 256, :], (((1,), (1,)), ((), ())), preferred_element_type=F32
        ).astype(BF)
        mine_ref[:, at : at + 256] = share[:half]
        other_ref[:, at : at + 256] = share[half:]


def down(hidden, w):
    rows, out = hidden.shape[0], w.shape[0]
    return pl.pallas_call(
        down_kernel,
        out_shape=(jax.ShapeDtypeStruct((rows // 2, out), BF),) * 2,
        in_specs=[VMEM, VMEM],
        out_specs=(VMEM, VMEM),
        compiler_params=limit(14),
        cost_estimate=pl.CostEstimate(
            flops=2 * rows * out * w.shape[1], bytes_accessed=4 << 20, transcendentals=0
        ),
        name="down",
    )(hidden, w)


def mixer_kernel(kind_ref, mine_ref, other_ref, w_ref, pool_ref, scale_ref, keep_ref, send_ref):
    rows = 2 * mine_ref.shape[0]
    tile = rows // 8
    kind, core = kind_ref[0], kind_ref[1]
    x = jnp.concatenate([mine_ref[...], other_ref[...]], axis=0)
    values = jnp.dot(x, w_ref[:, 0:128], preferred_element_type=F32)
    values = values.astype(BF).astype(F32)
    in_order = []
    for i in range(4):
        mine = values[i * tile : (i + 1) * tile]
        other = values[(4 + i) * tile : (5 + i) * tile]
        in_order += [jnp.where(core == 0, mine, other), jnp.where(core == 0, other, mine)]
    values = jnp.concatenate(in_order, axis=0)
    place = lax.broadcasted_iota(jnp.int32, (rows, 128), 0) % LEN
    total = values
    chosen = jnp.zeros_like(values)
    for slot in range(4):
        lag = 2**slot
        earlier = jnp.concatenate([jnp.zeros((lag, 128), F32), total[: rows - lag]], axis=0)
        total = total + jnp.where(place >= lag, earlier, 0.0)
        window = 2 * lag
        mean = total / jnp.minimum(place + 1, window).astype(F32)
        chosen = jnp.where(kind == slot, mean, chosen)
    deviation = (chosen - values).astype(BF)
    mixed = jnp.dot(deviation, pool_ref[...], preferred_element_type=F32)
    mixed = mixed * scale_ref[...].astype(F32)
    mixed = by_core(core, [mixed[i * tile : (i + 1) * tile] for i in range(8)]).astype(BF)
    for at in range(0, w_ref.shape[0], 256):
        share = lax.dot_general(
            mixed, w_ref[at : at + 256, 128:256], (((1,), (1,)), ((), ())), preferred_element_type=F32
        ).astype(BF)
        keep_ref[:, at : at + 256] = share[: rows // 2]
        send_ref[:, at : at + 256] = share[rows // 2 :]


def mixer(kind, mine, other, w, pool_w, pool_scale):
    rows, depth = 2 * mine.shape[0], mine.shape[1]
    return pl.pallas_call(
        mixer_kernel,
        out_shape=(jax.ShapeDtypeStruct((rows // 2, depth), BF),) * 2,
        in_specs=[SMEM] + [VMEM] * 5,
        out_specs=(VMEM, VMEM),
        compiler_params=limit(14),
        cost_estimate=pl.CostEstimate(
            flops=4 * rows * depth * 128, bytes_accessed=4 << 20, transcendentals=0
        ),
        name="mixer",
    )(kind, mine, other, w, pool_w, pool_scale)


X_GROUPS = [[2 * x + core for x in range(4)] for core in range(2)]


def core_swap(array):
    return lax.ppermute(array, "tp", [(k, k ^ 1) for k in range(8)])


def shares_of_rows(mine, other):
    both = (mine.astype(F32) + core_swap(other).astype(F32)).astype(BF)
    tiles = both.reshape(4, both.shape[0] // 4, both.shape[1])
    return lax.all_to_all(tiles, "tp", 0, 0, tiled=True, axis_index_groups=X_GROUPS)


def rows_of_all(normed):
    mine = lax.all_gather(normed, "tp", axis=0, tiled=True, axis_index_groups=X_GROUPS)
    return mine, core_swap(mine)


def body(tokens, w_gate, w_up, w_down, w_mix_in, w_mix_out, pool_w, pool_scale, norm_gains):
    tp_size, tp_at = lax.axis_size("tp"), lax.axis_index("tp")
    fs_at = lax.axis_index("fs")
    z, y = fs_at // NY, fs_at % NY
    own_rows = tokens.shape[0] // tp_size
    width = w_gate.shape[1]

    groups = [[k * NY + j for j in range(NY)] for k in range(NZ)]
    second_width = 256 + width
    first, second = pack(w_gate, w_up, w_mix_in, w_mix_out.T, w_down.T)
    first = lax.all_gather(first, "fs", axis=0, tiled=True, axis_index_groups=groups)

    first_block = lax.rem(z + 8, NZ)
    core = lax.rem(tp_at, 2)
    gains = rolled(norm_gains, first_block)
    gain = [gains[k : k + 1] for k in range(6)]
    numbers = jnp.stack([first_block, core, lax.rem(tp_at, 4), y]).astype(jnp.int32)

    back = ahead = jnp.concatenate([first, second], axis=0)
    got = {0: back}
    for k in range(1, 9):
        if k == 7:
            last_second = shift(back[128:, :second_width], dz=2)
        back = got[-k] = shift(back if k < 8 else back[:128], dz=1)
        if k < 8:
            ahead = got[k] = shift(ahead, dz=-1)
        if k == 2:
            back, late_tokens = lax.optimization_barrier((back, tokens))
            x = first_norm(numbers[0:2], late_tokens, gain[0])
        if k == 5:
            back, x = lax.optimization_barrier((back, x))
        got[-k] = back
    payloads = [got[k] for k in OFFSETS]

    late = ()
    for batch in BATCHES:
        own = [last_second if s == -8 else got[s][128:, :second_width] for s in batch]
        own = jnp.concatenate(own, axis=0)
        pieces = [own, shift(own, dy=1), shift(own, dy=2), shift(own, dy=-1)]
        late = assemble(numbers[3:4], pieces, batch, width, late)
    mix_w, down_w = late

    stream = lax.dynamic_slice_in_dim(tokens, tp_at * own_rows, own_rows, 0)
    stream = rolled(stream, first_block).astype(F32)
    parts = shares_of_rows(*down(gated([x], payloads, width), down_w))
    stream, normed = settle(parts, stream, gain[1], gain[2], 0.5)
    kind = jnp.stack([numbers[2], numbers[1]])
    share = mixer(kind, *rows_of_all(normed), mix_w, pool_w[0], pool_scale[None])
    stream, normed = settle(shares_of_rows(*share), stream, gain[3], gain[4], 1.0)
    hidden = gated(rows_of_all(normed), payloads, width)
    parts = shares_of_rows(*down(hidden, down_w))
    return finish(numbers[0:1], parts, stream, gain[5])


def solution(mesh):
    in_specs = (
        P("fs", None),
        P("fs", "tp"),
        P("fs", "tp"),
        P("tp", "fs"),
        P("fs", "tp"),
        P("tp", "fs"),
        P("tp", None, None),
        P("tp"),
        P(),
    )
    out_specs = P(("fs", "tp"), None)

    return jax.shard_map(body, mesh=mesh, in_specs=in_specs, out_specs=out_specs, check_vma=False)
```

```python
import functools

import jax
import jax.numpy as jnp
from jax import lax
from jax.experimental import pallas as pl
from jax.experimental.pallas import tpu as pltpu
from jax.sharding import PartitionSpec as P


LEN = 64
NZ, NY = 16, 4
BF = jnp.bfloat16
F32 = jnp.float32
VMEM = pl.BlockSpec(memory_space=pltpu.VMEM)
SMEM = pl.BlockSpec(memory_space=pltpu.SMEM)


LARGE = 63


def limit(mib):
    return pltpu.CompilerParams(vmem_limit_bytes=mib * 1024 * 1024)


OFFSETS = tuple(range(-8, 8))
BATCHES = ((0, -1, 1, -2, 2, -3, 3, -4, 4, -5, 5), (-6, 6, -7, 7, -8))
HBM = pl.BlockSpec(memory_space=pltpu.HBM)


def fs_shift(dy, dz):
    return [
        (z * NY + y, ((z + dz) % NZ) * NY + (y + dy) % NY) for z in range(NZ) for y in range(NY)
    ]


def shift(array, dy=0, dz=0):
    return lax.ppermute(array, "fs", fs_shift(dy, dz))


def rolled(array, first_block):
    twice = jnp.concatenate([array, array], axis=1)
    return lax.dynamic_slice_in_dim(twice, first_block * 128, array.shape[1], 1)


def pack_kernel(gate_in, up_in, mix_in, mix_out, down_in, first_ref, second_ref, *scratch):
    held, sems = scratch[:5], scratch[5]
    copies = []
    for k, (src, dst) in enumerate(zip((gate_in, up_in, mix_in, mix_out, down_in), held)):
        copies.append(pltpu.make_async_copy(src, dst, sems.at[k]))
        copies[-1].start()
    for copy in copies:
        copy.wait()
    gate_ref, up_ref, in_ref, out_ref, down_ref = held
    width = gate_ref.shape[1]
    whole = width // 128 * 128
    first_ref[:, :whole] = gate_ref[:, :whole]
    first_ref[:, whole : 2 * whole] = up_ref[:, :whole]
    first_ref[:, 2 * whole :] = jnp.concatenate([gate_ref[:, whole:], up_ref[:, whole:]], axis=1)
    second_ref[:, 0:128] = in_ref[...]
    second_ref[:, 128:256] = out_ref[...]
    second_ref[:, 256 : 256 + width] = down_ref[...]
    second_ref[:, 256 + width :] = jnp.zeros((32, width - 256), BF)


def pack(*weights):
    shape = jax.ShapeDtypeStruct((32, 2 * weights[0].shape[1]), BF)
    return pl.pallas_call(
        pack_kernel,
        out_shape=(shape, shape),
        in_specs=[HBM] * 5,
        out_specs=(VMEM, VMEM),
        scratch_shapes=[pltpu.VMEM(w.shape, BF) for w in weights] + [pltpu.SemaphoreType.DMA((5,))],
        compiler_params=limit(63),
        cost_estimate=pl.CostEstimate(flops=10**8, bytes_accessed=1 << 18, transcendentals=0),
        name="pack",
    )(*weights)


def by_core(core, blocks):
    even, odd = blocks[0::2], blocks[1::2]
    mine = [jnp.where(core == 0, a, b) for a, b in zip(even, odd)]
    other = [jnp.where(core == 0, b, a) for a, b in zip(even, odd)]
    return jnp.concatenate(mine + other, axis=0)


def first_norm_kernel(at_ref, x_ref, gain_ref, out_ref):
    rows, depth = x_ref.shape
    tile = rows // 8
    block, core = at_ref[0], at_ref[1]
    halves = ([], [])
    for i in range(4):
        x0 = x_ref[2 * i * tile : (2 * i + 1) * tile, :].astype(F32)
        x1 = x_ref[(2 * i + 1) * tile : (2 * i + 2) * tile, :].astype(F32)
        for k, x in enumerate((x0, x1)):
            scale = lax.rsqrt(jnp.mean(x * x, axis=-1, keepdims=True) + 1e-06)
            halves[k].append(scale)
    for p in range(depth // 128):
        start = pl.multiple_of(lax.rem(block + p, depth // 128) * 128, 128)
        gain = gain_ref[0:1, p * 128 : (p + 1) * 128]
        mine, other = [], []
        for i in range(4):
            x0 = x_ref[2 * i * tile : (2 * i + 1) * tile, pl.ds(start, 128)].astype(F32)
            x1 = x_ref[(2 * i + 1) * tile : (2 * i + 2) * tile, pl.ds(start, 128)].astype(F32)
            x0 = (x0 * halves[0][i] * gain).astype(BF)
            x1 = (x1 * halves[1][i] * gain).astype(BF)
            mine.append(jnp.where(core == 0, x0, x1))
            other.append(jnp.where(core == 0, x1, x0))
        for i in range(4):
            out_ref[i * tile : (i + 1) * tile, p * 128 : (p + 1) * 128] = mine[i]
            out_ref[(4 + i) * tile : (5 + i) * tile, p * 128 : (p + 1) * 128] = other[i]


def first_norm(at, tokens, gain):
    return pl.pallas_call(
        first_norm_kernel,
        out_shape=jax.ShapeDtypeStruct(tokens.shape, BF),
        in_specs=[SMEM, VMEM, VMEM],
        out_specs=VMEM,
        compiler_params=limit(8),
        cost_estimate=pl.CostEstimate(flops=10**9, bytes_accessed=3 << 20, transcendentals=0),
        name="first_norm",
    )(at, tokens, gain)


def rms_scale(values, gain):
    return values * lax.rsqrt(jnp.mean(values * values, axis=-1, keepdims=True) + 1e-06) * gain


def settle_kernel(factor, row, parts_ref, stream_ref, gain_ref, new_ref, normed_ref):
    total = parts_ref[0].astype(F32)
    for k in range(1, parts_ref.shape[0]):
        total = total + parts_ref[k].astype(F32)
    stream = stream_ref[...] + factor * rms_scale(total, gain_ref[row : row + 1, :])
    new_ref[...] = stream
    normed = rms_scale(stream, gain_ref[row + 1 : row + 2, :]).astype(BF)
    for k in range(normed_ref.shape[0]):
        normed_ref[k] = normed


def settle(parts, stream, gains, row, factor):
    return pl.pallas_call(
        functools.partial(settle_kernel, factor, row),
        out_shape=(
            jax.ShapeDtypeStruct(stream.shape, F32),
            jax.ShapeDtypeStruct((4, *stream.shape), BF),
        ),
        in_specs=[VMEM] * 3,
        out_specs=(VMEM, VMEM),
        compiler_params=limit(6),
        cost_estimate=pl.CostEstimate(flops=10**8, bytes_accessed=1 << 20, transcendentals=0),
        name="settle",
    )(parts, stream, gains)


def finish_kernel(at_ref, parts_ref, stream_ref, gain_ref, out_ref):
    total = parts_ref[0].astype(F32)
    for k in range(1, parts_ref.shape[0]):
        total = total + parts_ref[k].astype(F32)
    result = (stream_ref[...] + 0.5 * rms_scale(total, gain_ref[5:6, :])).astype(BF)
    blocks = result.shape[1] // 128
    for p in range(blocks):
        start = pl.multiple_of(lax.rem(at_ref[0] + p, blocks) * 128, 128)
        out_ref[:, pl.ds(start, 128)] = result[:, p * 128 : (p + 1) * 128]


def finish(at, parts, stream, gains):
    return pl.pallas_call(
        finish_kernel,
        out_shape=jax.ShapeDtypeStruct(stream.shape, BF),
        in_specs=[SMEM] + [VMEM] * 3,
        out_specs=VMEM,
        compiler_params=limit(6),
        cost_estimate=pl.CostEstimate(flops=10**8, bytes_accessed=1 << 20, transcendentals=0),
        name="finish",
    )(at, parts, stream, gains)


def act(gate, up):
    return (gate / (1.0 + jnp.exp(-gate)) * up).astype(BF)


def gated_kernel(width, parts, *refs):
    ins, out_ref = refs[: parts + NZ], refs[parts + NZ]
    x_ref, w_ref, total_ref, sems = refs[parts + NZ + 1 :]
    copies, at = [], 0
    for k in range(parts):
        rows = ins[k].shape[0]
        copies.append(pltpu.make_async_copy(ins[k], x_ref.at[at : at + rows], sems.at[k]))
        at += rows
    for k in range(NZ):
        rows = w_ref.at[k * 128 : (k + 1) * 128]
        src = ins[parts + k].at[0:128]
        copies.append(pltpu.make_async_copy(src, rows, sems.at[parts + k]))
    for copy in copies:
        copy.start()
    for copy in copies[:parts]:
        copy.wait()
    step = 4
    for k in range(0, NZ, step):
        for copy in copies[parts + k : parts + k + step]:
            copy.wait()
        deep = slice(k * 128, (k + step) * 128)
        for at in range(0, 2 * width, 256):
            end = min(at + 256, 2 * width)
            part = jnp.dot(x_ref[:, deep], w_ref[deep, at:end], preferred_element_type=F32)
            total_ref[:, at:end] = part if k == 0 else total_ref[:, at:end] + part
    whole = width // 128 * 128
    out_ref[:, :whole] = act(total_ref[:, :whole], total_ref[:, whole : 2 * whole])
    both = total_ref[:, 2 * whole :]
    out_ref[:, whole:] = act(both[:, : width - whole], both[:, width - whole :])


def gated(xs, payloads, width):
    rows, depth = sum(x.shape[0] for x in xs), xs[0].shape[1]
    return pl.pallas_call(
        functools.partial(gated_kernel, width, len(xs)),
        out_shape=jax.ShapeDtypeStruct((rows, width), BF),
        in_specs=[HBM] * (len(xs) + NZ),
        out_specs=VMEM,
        scratch_shapes=[
            pltpu.VMEM((rows, depth), BF),
            pltpu.VMEM((depth, 2 * width), BF),
            pltpu.VMEM((rows, 2 * width), F32),
            pltpu.SemaphoreType.DMA((len(xs) + NZ,)),
        ],
        compiler_params=limit(LARGE),
        cost_estimate=pl.CostEstimate(
            flops=4 * rows * depth * width, bytes_accessed=8 << 20, transcendentals=0
        ),
        name="gated",
    )(*xs, *payloads)


def collect_kernel(*refs):
    ins, out_ref, held_ref, sems = refs[:-3], refs[-3], refs[-2], refs[-1]
    copies = []
    for k, ref in enumerate(ins):
        rows = held_ref.at[k * 32 : (k + 1) * 32]
        if ref.shape[0] == 32:
            copies.append(pltpu.make_async_copy(ref, rows, sems.at[k]))
        else:
            copies.append(pltpu.make_async_copy(ref.at[128:160], rows, sems.at[k]))
        copies[-1].start()
    for copy in copies:
        copy.wait()
    out_ref[...] = held_ref[:, 0 : out_ref.shape[1]]


def collect(blocks, width):
    rows = 32 * len(blocks)
    return pl.pallas_call(
        collect_kernel,
        out_shape=jax.ShapeDtypeStruct((rows, width), BF),
        in_specs=[HBM] * len(blocks),
        out_specs=VMEM,
        scratch_shapes=[
            pltpu.VMEM((rows, blocks[0].shape[1]), BF),
            pltpu.SemaphoreType.DMA((len(blocks),)),
        ],
        compiler_params=limit(LARGE),
        cost_estimate=pl.CostEstimate(flops=10**8, bytes_accessed=1 << 20, transcendentals=0),
        name="collect",
    )(*blocks)


def gather_copies(y, pieces, held_ref, sems, columns):
    copies = {}
    for b, batch in enumerate(BATCHES):
        for j in range(NY):
            owner = lax.rem(y - j + NY, NY)
            for i, offset in enumerate(batch):
                p = OFFSETS.index(offset)
                start = pl.multiple_of(p * 128 + owner * 32, 32)
                src = pieces[NY * b + j]
                if columns is None:
                    src = src.at[i * 32 : (i + 1) * 32]
                else:
                    src = src.at[i * 32 : (i + 1) * 32, 0:columns]
                rows = held_ref.at[pl.ds(start, 32)]
                copies[p, j] = pltpu.make_async_copy(src, rows, sems.at[p * NY + j])
    for p in range(NZ):
        for j in range(NY):
            copies[p, j].start()
    return copies


def down_kernel(y_ref, h_ref, *refs):
    pieces, mine_ref, other_ref, held_ref, sems = refs[:-4], refs[-4], refs[-3], refs[-2], refs[-1]
    copies = gather_copies(y_ref[0], pieces, held_ref, sems, None)
    h = h_ref[...]
    half = h.shape[0] // 2
    for at in range(0, held_ref.shape[0], 256):
        for p in range(at // 128, at // 128 + 2):
            for j in range(NY):
                copies[p, j].wait()
        share = lax.dot_general(
            h, held_ref[at : at + 256, 256:], (((1,), (1,)), ((), ())), preferred_element_type=F32
        ).astype(BF)
        mine_ref[:, at : at + 256] = share[:half]
        other_ref[:, at : at + 256] = share[half:]


def down(y, hidden, pieces):
    rows, out = hidden.shape[0], NZ * NY * 32
    return pl.pallas_call(
        down_kernel,
        out_shape=(jax.ShapeDtypeStruct((rows // 2, out), BF),) * 2,
        in_specs=[SMEM, VMEM] + [HBM] * len(pieces),
        out_specs=(VMEM, VMEM),
        scratch_shapes=[
            pltpu.VMEM((out, pieces[0].shape[1]), BF),
            pltpu.SemaphoreType.DMA((NZ * NY,)),
        ],
        compiler_params=limit(LARGE - 2),
        cost_estimate=pl.CostEstimate(
            flops=2 * rows * out * hidden.shape[1], bytes_accessed=4 << 20, transcendentals=0
        ),
        name="down",
    )(y, hidden, *pieces)


def mixer_kernel(kind_ref, mine_ref, other_ref, pool_ref, scale_ref, *refs):
    pieces, keep_ref, send_ref, w_ref, sems = refs[:-4], refs[-4], refs[-3], refs[-2], refs[-1]
    copies = gather_copies(kind_ref[2], pieces, w_ref, sems, 256)
    for copy in copies.values():
        copy.wait()
    rows = 2 * mine_ref.shape[0]
    tile = rows // 8
    kind, core = kind_ref[0], kind_ref[1]
    x = jnp.concatenate([mine_ref[...], other_ref[...]], axis=0)
    values = jnp.dot(x, w_ref[:, 0:128], preferred_element_type=F32)
    values = values.astype(BF).astype(F32)
    in_order = []
    for i in range(4):
        mine = values[i * tile : (i + 1) * tile]
        other = values[(4 + i) * tile : (5 + i) * tile]
        in_order += [jnp.where(core == 0, mine, other), jnp.where(core == 0, other, mine)]
    values = jnp.concatenate(in_order, axis=0)
    place = lax.broadcasted_iota(jnp.int32, (rows, 128), 0) % LEN
    total = values
    chosen = jnp.zeros_like(values)
    for slot in range(4):
        lag = 2**slot
        earlier = jnp.concatenate([jnp.zeros((lag, 128), F32), total[: rows - lag]], axis=0)
        total = total + jnp.where(place >= lag, earlier, 0.0)
        window = 2 * lag
        mean = total / jnp.minimum(place + 1, window).astype(F32)
        chosen = jnp.where(kind == slot, mean, chosen)
    deviation = (chosen - values).astype(BF)
    mixed = jnp.dot(deviation, pool_ref[...], preferred_element_type=F32)
    mixed = mixed * scale_ref[...].astype(F32)
    mixed = by_core(core, [mixed[i * tile : (i + 1) * tile] for i in range(8)]).astype(BF)
    for at in range(0, w_ref.shape[0], 256):
        share = lax.dot_general(
            mixed, w_ref[at : at + 256, 128:256], (((1,), (1,)), ((), ())), preferred_element_type=F32
        ).astype(BF)
        keep_ref[:, at : at + 256] = share[: rows // 2]
        send_ref[:, at : at + 256] = share[rows // 2 :]


def mixer(kind, mine, other, pool_w, pool_scale, pieces):
    rows, depth = 2 * mine.shape[0], mine.shape[1]
    return pl.pallas_call(
        mixer_kernel,
        out_shape=(jax.ShapeDtypeStruct((rows // 2, depth), BF),) * 2,
        in_specs=[SMEM] + [VMEM] * 4 + [HBM] * len(pieces),
        out_specs=(VMEM, VMEM),
        scratch_shapes=[pltpu.VMEM((depth, 256), BF), pltpu.SemaphoreType.DMA((NZ * NY,))],
        compiler_params=limit(LARGE - 4),
        cost_estimate=pl.CostEstimate(
            flops=4 * rows * depth * 128, bytes_accessed=4 << 20, transcendentals=0
        ),
        name="mixer",
    )(kind, mine, other, pool_w, pool_scale, *pieces)


X_GROUPS = [[2 * x + core for x in range(4)] for core in range(2)]


def core_swap(array):
    return lax.ppermute(array, "tp", [(k, k ^ 1) for k in range(8)])


def shares_of_rows(mine, other):
    both = (mine.astype(F32) + core_swap(other).astype(F32)).astype(BF)
    tiles = both.reshape(4, both.shape[0] // 4, both.shape[1])
    return lax.all_to_all(tiles, "tp", 0, 0, tiled=True, axis_index_groups=X_GROUPS)


def rows_of_all(copies):
    mine = lax.all_to_all(copies, "tp", 0, 0, tiled=True, axis_index_groups=X_GROUPS)
    mine = mine.reshape(-1, copies.shape[-1])
    return mine, core_swap(mine)


def body(tokens, w_gate, w_up, w_down, w_mix_in, w_mix_out, pool_w, pool_scale, norm_gains):
    tp_size, tp_at = lax.axis_size("tp"), lax.axis_index("tp")
    fs_at = lax.axis_index("fs")
    z, y = fs_at // NY, fs_at % NY
    own_rows = tokens.shape[0] // tp_size
    width = w_gate.shape[1]

    groups = [[k * NY + j for j in range(NY)] for k in range(NZ)]
    second_width = 256 + width
    first, second = pack(w_gate, w_up, w_mix_in, w_mix_out.T, w_down.T)
    first = lax.all_gather(first, "fs", axis=0, tiled=True, axis_index_groups=groups)

    first_block = lax.rem(z + 8, NZ)
    core = lax.rem(tp_at, 2)
    gains = rolled(norm_gains, first_block)
    numbers = jnp.stack([first_block, core, lax.rem(tp_at, 4), y]).astype(jnp.int32)

    back = ahead = jnp.concatenate([first, second], axis=0)
    got = {0: back}
    for k in range(1, 9):
        if k == 7:
            last_second = shift(back[128:], dz=2)
        back = got[-k] = shift(back, dz=1)
        if k < 8:
            ahead = got[k] = shift(ahead, dz=-1)
        if k == 2:
            back, late_tokens = lax.optimization_barrier((back, tokens))
            x = first_norm(numbers[0:2], late_tokens, gains)
        if k == 5:
            back, x = lax.optimization_barrier((back, x))
        got[-k] = back
    payloads = [got[k] for k in OFFSETS]

    pieces = []
    for batch in BATCHES:
        own = collect([last_second if s == -8 else got[s] for s in batch], second_width)
        pieces += [own, shift(own, dy=1), shift(own, dy=2), shift(own, dy=-1)]

    stream = lax.dynamic_slice_in_dim(tokens, tp_at * own_rows, own_rows, 0)
    stream = rolled(stream, first_block).astype(F32)
    hidden = gated([x], payloads, width)
    parts = shares_of_rows(*down(numbers[3:4], hidden, pieces))
    stream, copies = settle(parts, stream, gains, 1, 0.5)
    kind = jnp.stack([numbers[2], numbers[1], numbers[3]])
    share = mixer(kind, *rows_of_all(copies), pool_w[0], pool_scale[None], pieces)
    stream, copies = settle(shares_of_rows(*share), stream, gains, 3, 1.0)
    hidden = gated(rows_of_all(copies), payloads, width)
    parts = shares_of_rows(*down(numbers[3:4], hidden, pieces))
    return finish(numbers[0:1], parts, stream, gains)


def solution(mesh):
    in_specs = (
        P("fs", None),
        P("fs", "tp"),
        P("fs", "tp"),
        P("tp", "fs"),
        P("fs", "tp"),
        P("tp", "fs"),
        P("tp", None, None),
        P("tp"),
        P(),
    )
    out_specs = P(("fs", "tp"), None)

    return jax.shard_map(body, mesh=mesh, in_specs=in_specs, out_specs=out_specs, check_vma=False)
```

```python
import functools

import jax
import jax.numpy as jnp
from jax import lax
from jax.experimental import pallas as pl
from jax.experimental.pallas import tpu as pltpu
from jax.sharding import PartitionSpec as P


LEN = 64
NZ, NY = 16, 4
BF = jnp.bfloat16
F32 = jnp.float32
VMEM = pl.BlockSpec(memory_space=pltpu.VMEM)
SMEM = pl.BlockSpec(memory_space=pltpu.SMEM)


def limit(mib):
    return pltpu.CompilerParams(vmem_limit_bytes=mib * 1024 * 1024)


OFFSETS = tuple(range(-8, 8))
BATCHES = ((0, -1, 1, -2, 2, -3, 3, -4, 4, -5, 5), (-6, 6, -7, 7, -8))
HBM = pl.BlockSpec(memory_space=pltpu.HBM)


def fs_shift(dy, dz):
    return [
        (z * NY + y, ((z + dz) % NZ) * NY + (y + dy) % NY) for z in range(NZ) for y in range(NY)
    ]


def shift(array, dy=0, dz=0):
    return lax.ppermute(array, "fs", fs_shift(dy, dz))


def rolled(array, first_block):
    twice = jnp.concatenate([array, array], axis=1)
    return lax.dynamic_slice_in_dim(twice, first_block * 128, array.shape[1], 1)


def pack_kernel(gate_in, up_in, mix_in, mix_out, down_in, first_ref, second_ref, *scratch):
    held, sems = scratch[:5], scratch[5]
    copies = []
    for k, (src, dst) in enumerate(zip((gate_in, up_in, mix_in, mix_out, down_in), held)):
        copies.append(pltpu.make_async_copy(src, dst, sems.at[k]))
        copies[-1].start()
    for copy in copies:
        copy.wait()
    gate_ref, up_ref, in_ref, out_ref, down_ref = held
    width = gate_ref.shape[1]
    whole = width // 128 * 128
    first_ref[:, :whole] = gate_ref[:, :whole]
    first_ref[:, whole : 2 * whole] = up_ref[:, :whole]
    first_ref[:, 2 * whole :] = jnp.concatenate([gate_ref[:, whole:], up_ref[:, whole:]], axis=1)
    second_ref[:, 0:128] = in_ref[...]
    second_ref[:, 128:256] = out_ref[...]
    second_ref[:, 256 : 256 + width] = down_ref[...]
    second_ref[:, 256 + width :] = jnp.zeros((32, width - 256), BF)


def pack(*weights):
    shape = jax.ShapeDtypeStruct((32, 2 * weights[0].shape[1]), BF)
    return pl.pallas_call(
        pack_kernel,
        out_shape=(shape, shape),
        in_specs=[HBM] * 5,
        out_specs=(VMEM, VMEM),
        scratch_shapes=[pltpu.VMEM(w.shape, BF) for w in weights] + [pltpu.SemaphoreType.DMA((5,))],
        compiler_params=limit(63),
        cost_estimate=pl.CostEstimate(flops=10**8, bytes_accessed=1 << 18, transcendentals=0),
        name="pack",
    )(*weights)


def by_core(core, blocks):
    even, odd = blocks[0::2], blocks[1::2]
    mine = [jnp.where(core == 0, a, b) for a, b in zip(even, odd)]
    other = [jnp.where(core == 0, b, a) for a, b in zip(even, odd)]
    return jnp.concatenate(mine + other, axis=0)


def first_norm_kernel(at_ref, x_ref, gain_ref, out_ref):
    rows, depth = x_ref.shape
    tile = rows // 8
    block, core = at_ref[0], at_ref[1]
    halves = ([], [])
    for i in range(4):
        x0 = x_ref[2 * i * tile : (2 * i + 1) * tile, :].astype(F32)
        x1 = x_ref[(2 * i + 1) * tile : (2 * i + 2) * tile, :].astype(F32)
        for k, x in enumerate((x0, x1)):
            scale = lax.rsqrt(jnp.mean(x * x, axis=-1, keepdims=True) + 1e-06)
            halves[k].append(scale)
    for p in range(depth // 128):
        start = pl.multiple_of(lax.rem(block + p, depth // 128) * 128, 128)
        gain = gain_ref[0:1, p * 128 : (p + 1) * 128]
        mine, other = [], []
        for i in range(4):
            x0 = x_ref[2 * i * tile : (2 * i + 1) * tile, pl.ds(start, 128)].astype(F32)
            x1 = x_ref[(2 * i + 1) * tile : (2 * i + 2) * tile, pl.ds(start, 128)].astype(F32)
            x0 = (x0 * halves[0][i] * gain).astype(BF)
            x1 = (x1 * halves[1][i] * gain).astype(BF)
            mine.append(jnp.where(core == 0, x0, x1))
            other.append(jnp.where(core == 0, x1, x0))
        for i in range(4):
            out_ref[i * tile : (i + 1) * tile, p * 128 : (p + 1) * 128] = mine[i]
            out_ref[(4 + i) * tile : (5 + i) * tile, p * 128 : (p + 1) * 128] = other[i]


def first_norm(at, tokens, gain):
    return pl.pallas_call(
        first_norm_kernel,
        out_shape=jax.ShapeDtypeStruct(tokens.shape, BF),
        in_specs=[SMEM, VMEM, VMEM],
        out_specs=VMEM,
        compiler_params=limit(8),
        cost_estimate=pl.CostEstimate(flops=10**9, bytes_accessed=3 << 20, transcendentals=0),
        name="first_norm",
    )(at, tokens, gain)


def rms_scale(values, gain):
    return values * lax.rsqrt(jnp.mean(values * values, axis=-1, keepdims=True) + 1e-06) * gain


def settle_kernel(factor, row, parts_ref, stream_ref, gain_ref, new_ref, normed_ref):
    total = parts_ref[0].astype(F32)
    for k in range(1, parts_ref.shape[0]):
        total = total + parts_ref[k].astype(F32)
    stream = stream_ref[...] + factor * rms_scale(total, gain_ref[row : row + 1, :])
    new_ref[...] = stream
    normed = rms_scale(stream, gain_ref[row + 1 : row + 2, :]).astype(BF)
    for k in range(normed_ref.shape[0]):
        normed_ref[k] = normed


def settle(parts, stream, gains, row, factor):
    return pl.pallas_call(
        functools.partial(settle_kernel, factor, row),
        out_shape=(
            jax.ShapeDtypeStruct(stream.shape, F32),
            jax.ShapeDtypeStruct((4, *stream.shape), BF),
        ),
        in_specs=[VMEM] * 3,
        out_specs=(VMEM, VMEM),
        compiler_params=limit(6),
        cost_estimate=pl.CostEstimate(flops=10**8, bytes_accessed=1 << 20, transcendentals=0),
        name="settle",
    )(parts, stream, gains)


def finish_kernel(at_ref, parts_ref, stream_ref, gain_ref, out_ref):
    total = parts_ref[0].astype(F32)
    for k in range(1, parts_ref.shape[0]):
        total = total + parts_ref[k].astype(F32)
    result = (stream_ref[...] + 0.5 * rms_scale(total, gain_ref[5:6, :])).astype(BF)
    blocks = result.shape[1] // 128
    for p in range(blocks):
        start = pl.multiple_of(lax.rem(at_ref[0] + p, blocks) * 128, 128)
        out_ref[:, pl.ds(start, 128)] = result[:, p * 128 : (p + 1) * 128]


def finish(at, parts, stream, gains):
    return pl.pallas_call(
        finish_kernel,
        out_shape=jax.ShapeDtypeStruct(stream.shape, BF),
        in_specs=[SMEM] + [VMEM] * 3,
        out_specs=VMEM,
        compiler_params=limit(6),
        cost_estimate=pl.CostEstimate(flops=10**8, bytes_accessed=1 << 20, transcendentals=0),
        name="finish",
    )(at, parts, stream, gains)


def act(gate, up):
    return (gate / (1.0 + jnp.exp(-gate)) * up).astype(BF)


def gated_kernel(width, parts, *refs):
    payloads, out_ref, w_ref = refs[parts : parts + NZ], refs[-2], refs[-1]
    for k in range(NZ):
        w_ref[k * 128 : (k + 1) * 128, :] = payloads[k][0:128, :]
    x = jnp.concatenate([ref[...] for ref in refs[:parts]], axis=0)
    whole = width // 128 * 128
    at = 0
    while at < whole:
        n = min(256, whole - at)
        gate = jnp.dot(x, w_ref[:, at : at + n], preferred_element_type=F32)
        up = jnp.dot(x, w_ref[:, whole + at : whole + at + n], preferred_element_type=F32)
        out_ref[:, at : at + n] = act(gate, up)
        at += n
    both = jnp.dot(x, w_ref[:, 2 * whole :], preferred_element_type=F32)
    out_ref[:, whole:] = act(both[:, : width - whole], both[:, width - whole :])


def gated(xs, payloads, width):
    rows, depth = sum(x.shape[0] for x in xs), xs[0].shape[1]
    return pl.pallas_call(
        functools.partial(gated_kernel, width, len(xs)),
        out_shape=jax.ShapeDtypeStruct((rows, width), BF),
        in_specs=[VMEM] * (len(xs) + NZ),
        out_specs=VMEM,
        scratch_shapes=[pltpu.VMEM((depth, 2 * width), BF)],
        compiler_params=limit(16),
        cost_estimate=pl.CostEstimate(
            flops=4 * rows * depth * width, bytes_accessed=8 << 20, transcendentals=0
        ),
        name="gated",
    )(*xs, *payloads)


def absorb_kernel(places, x_ref, *refs):
    n = len(places)
    blocks, total_ref = refs[:n], refs[-1]
    x = [x_ref[:, place * 128 : (place + 1) * 128] for place in places]
    x = x[0] if n == 1 else jnp.concatenate(x, axis=1)
    width = total_ref.shape[1]
    for at in range(0, width, 256):
        end = min(width, at + 256)
        w = [block[0:128, at:end] for block in blocks]
        w = w[0] if n == 1 else jnp.concatenate(w, axis=0)
        part = jnp.dot(x, w, preferred_element_type=F32)
        total_ref[:, at:end] = part if len(refs) == n + 1 else refs[n][:, at:end] + part


def absorb(x, blocks, places, total=None):
    rows, width, n = x.shape[0], blocks[0].shape[1], len(blocks)
    carried = () if total is None else (total,)
    return pl.pallas_call(
        functools.partial(absorb_kernel, places),
        out_shape=jax.ShapeDtypeStruct((rows, width), F32),
        in_specs=[VMEM] * (1 + n + len(carried)),
        out_specs=VMEM,
        input_output_aliases={} if total is None else {1 + n: 0},
        compiler_params=limit(6),
        cost_estimate=pl.CostEstimate(
            flops=2 * rows * width * 128 * n, bytes_accessed=n << 19, transcendentals=0
        ),
        name="absorb",
    )(x, *blocks, *carried)


def silu_kernel(total_ref, out_ref):
    width = out_ref.shape[1]
    whole = width // 128 * 128
    out_ref[:, :whole] = act(total_ref[:, :whole], total_ref[:, whole : 2 * whole])
    both = total_ref[:, 2 * whole :]
    out_ref[:, whole:] = act(both[:, : width - whole], both[:, width - whole :])


def silu(total):
    rows, width = total.shape
    return pl.pallas_call(
        silu_kernel,
        out_shape=jax.ShapeDtypeStruct((rows, width // 2), BF),
        in_specs=[VMEM],
        out_specs=VMEM,
        compiler_params=limit(4),
        cost_estimate=pl.CostEstimate(flops=10**8, bytes_accessed=1 << 20, transcendentals=0),
        name="silu",
    )(total)


def assemble_kernel(y_ref, *refs):
    ins, mix_ref, down_ref = refs[:-2], refs[-2], refs[-1]
    y = y_ref[0]
    width = mix_ref.shape[1] + down_ref.shape[1]
    for k, batch in enumerate(BATCHES):
        for j in range(NY):
            owner = lax.rem(y - j + NY, NY)
            src = ins[NY * k + j]
            for i, offset in enumerate(batch):
                start = pl.multiple_of(OFFSETS.index(offset) * 128 + owner * 32, 32)
                mix_ref[pl.ds(start, 32), :] = src[i * 32 : (i + 1) * 32, 0:256]
                down_ref[pl.ds(start, 32), :] = src[i * 32 : (i + 1) * 32, 256:width]


def assemble(y, pieces, down_width):
    rows = NZ * NY * 32
    return pl.pallas_call(
        assemble_kernel,
        out_shape=(
            jax.ShapeDtypeStruct((rows, 256), BF),
            jax.ShapeDtypeStruct((rows, down_width), BF),
        ),
        in_specs=[SMEM] + [VMEM] * len(pieces),
        out_specs=(VMEM, VMEM),
        compiler_params=limit(14),
        cost_estimate=pl.CostEstimate(flops=10**8, bytes_accessed=8 << 20, transcendentals=0),
        name="assemble",
    )(y, *pieces)


def down_kernel(h_ref, w_ref, mine_ref, other_ref):
    h = h_ref[...]
    half = h.shape[0] // 2
    for at in range(0, w_ref.shape[0], 256):
        share = lax.dot_general(
            h, w_ref[at : at + 256, :], (((1,), (1,)), ((), ())), preferred_element_type=F32
        ).astype(BF)
        mine_ref[:, at : at + 256] = share[:half]
        other_ref[:, at : at + 256] = share[half:]


def down(hidden, w):
    rows, out = hidden.shape[0], w.shape[0]
    return pl.pallas_call(
        down_kernel,
        out_shape=(jax.ShapeDtypeStruct((rows // 2, out), BF),) * 2,
        in_specs=[VMEM, VMEM],
        out_specs=(VMEM, VMEM),
        compiler_params=limit(14),
        cost_estimate=pl.CostEstimate(
            flops=2 * rows * out * w.shape[1], bytes_accessed=4 << 20, transcendentals=0
        ),
        name="down",
    )(hidden, w)


def mixer_kernel(kind_ref, mine_ref, other_ref, w_ref, pool_ref, scale_ref, keep_ref, send_ref):
    rows = 2 * mine_ref.shape[0]
    tile = rows // 8
    kind, core = kind_ref[0], kind_ref[1]
    x = jnp.concatenate([mine_ref[...], other_ref[...]], axis=0)
    values = jnp.dot(x, w_ref[:, 0:128], preferred_element_type=F32)
    values = values.astype(BF).astype(F32)
    in_order = []
    for i in range(4):
        mine = values[i * tile : (i + 1) * tile]
        other = values[(4 + i) * tile : (5 + i) * tile]
        in_order += [jnp.where(core == 0, mine, other), jnp.where(core == 0, other, mine)]
    values = jnp.concatenate(in_order, axis=0)
    place = lax.broadcasted_iota(jnp.int32, (rows, 128), 0) % LEN
    total = values
    chosen = jnp.zeros_like(values)
    for slot in range(4):
        lag = 2**slot
        earlier = jnp.concatenate([jnp.zeros((lag, 128), F32), total[: rows - lag]], axis=0)
        total = total + jnp.where(place >= lag, earlier, 0.0)
        window = 2 * lag
        mean = total / jnp.minimum(place + 1, window).astype(F32)
        chosen = jnp.where(kind == slot, mean, chosen)
    deviation = (chosen - values).astype(BF)
    mixed = jnp.dot(deviation, pool_ref[...], preferred_element_type=F32)
    mixed = mixed * scale_ref[...].astype(F32)
    mixed = by_core(core, [mixed[i * tile : (i + 1) * tile] for i in range(8)]).astype(BF)
    for at in range(0, w_ref.shape[0], 256):
        share = lax.dot_general(
            mixed, w_ref[at : at + 256, 128:256], (((1,), (1,)), ((), ())), preferred_element_type=F32
        ).astype(BF)
        keep_ref[:, at : at + 256] = share[: rows // 2]
        send_ref[:, at : at + 256] = share[rows // 2 :]


def mixer(kind, mine, other, w, pool_w, pool_scale):
    rows, depth = 2 * mine.shape[0], mine.shape[1]
    return pl.pallas_call(
        mixer_kernel,
        out_shape=(jax.ShapeDtypeStruct((rows // 2, depth), BF),) * 2,
        in_specs=[SMEM] + [VMEM] * 5,
        out_specs=(VMEM, VMEM),
        compiler_params=limit(14),
        cost_estimate=pl.CostEstimate(
            flops=4 * rows * depth * 128, bytes_accessed=4 << 20, transcendentals=0
        ),
        name="mixer",
    )(kind, mine, other, w, pool_w, pool_scale)


X_GROUPS = [[2 * x + core for x in range(4)] for core in range(2)]


def core_swap(array):
    return lax.ppermute(array, "tp", [(k, k ^ 1) for k in range(8)])


def shares_of_rows(mine, other):
    both = (mine.astype(F32) + core_swap(other).astype(F32)).astype(BF)
    tiles = both.reshape(4, both.shape[0] // 4, both.shape[1])
    return lax.all_to_all(tiles, "tp", 0, 0, tiled=True, axis_index_groups=X_GROUPS)


def rows_of_all(copies):
    mine = lax.all_to_all(copies, "tp", 0, 0, tiled=True, axis_index_groups=X_GROUPS)
    mine = mine.reshape(-1, copies.shape[-1])
    return mine, core_swap(mine)


def body(tokens, w_gate, w_up, w_down, w_mix_in, w_mix_out, pool_w, pool_scale, norm_gains):
    tp_size, tp_at = lax.axis_size("tp"), lax.axis_index("tp")
    fs_at = lax.axis_index("fs")
    z, y = fs_at // NY, fs_at % NY
    own_rows = tokens.shape[0] // tp_size
    width = w_gate.shape[1]

    groups = [[k * NY + j for j in range(NY)] for k in range(NZ)]
    second_width = 256 + width
    first, second = pack(w_gate, w_up, w_mix_in, w_mix_out.T, w_down.T)
    first = lax.all_gather(first, "fs", axis=0, tiled=True, axis_index_groups=groups)

    first_block = lax.rem(z + 8, NZ)
    core = lax.rem(tp_at, 2)
    gains = rolled(norm_gains, first_block)
    numbers = jnp.stack([first_block, core, lax.rem(tp_at, 4), y]).astype(jnp.int32)

    first, late_tokens = lax.optimization_barrier((first, tokens))
    back = ahead = jnp.concatenate([first, second], axis=0)
    x = first_norm(numbers[0:2], late_tokens, gains)
    got = {0: back}
    total = None
    for k in range(1, 9):
        if k == 7:
            last_second = shift(back[128:, :second_width], dz=2)
        back = got[-k] = shift(back, dz=1)
        if k < 8:
            ahead = got[k] = shift(ahead, dz=-1)
        places = ([0] if k == 1 else []) + [-k] + ([k] if k < 8 else [])
        total = absorb(x, [got[p] for p in places], tuple(8 + p for p in places), total)
    payloads = [got[k] for k in OFFSETS]

    pieces = []
    for batch in BATCHES:
        own = [last_second if s == -8 else got[s][128:, :second_width] for s in batch]
        own = jnp.concatenate(own, axis=0)
        pieces += [own, shift(own, dy=1), shift(own, dy=2), shift(own, dy=-1)]
    mix_w, down_w = assemble(numbers[3:4], pieces, width)

    stream = lax.dynamic_slice_in_dim(tokens, tp_at * own_rows, own_rows, 0)
    stream = rolled(stream, first_block).astype(F32)
    hidden = silu(total)
    parts = shares_of_rows(*down(hidden, down_w))
    stream, copies = settle(parts, stream, gains, 1, 0.5)
    kind = jnp.stack([numbers[2], numbers[1]])
    share = mixer(kind, *rows_of_all(copies), mix_w, pool_w[0], pool_scale[None])
    stream, copies = settle(shares_of_rows(*share), stream, gains, 3, 1.0)
    hidden = gated(rows_of_all(copies), payloads, width)
    parts = shares_of_rows(*down(hidden, down_w))
    return finish(numbers[0:1], parts, stream, gains)


def solution(mesh):
    in_specs = (
        P("fs", None),
        P("fs", "tp"),
        P("fs", "tp"),
        P("tp", "fs"),
        P("fs", "tp"),
        P("tp", "fs"),
        P("tp", None, None),
        P("tp"),
        P(),
    )
    out_specs = P(("fs", "tp"), None)

    return jax.shard_map(body, mesh=mesh, in_specs=in_specs, out_specs=out_specs, check_vma=False)
```

```python
import functools

import jax
import jax.numpy as jnp
from jax import lax
from jax.experimental import pallas as pl
from jax.experimental.pallas import tpu as pltpu
from jax.sharding import PartitionSpec as P


LEN = 64
NZ, NY = 16, 4
SECOND = 1280
BF = jnp.bfloat16
F32 = jnp.float32
VMEM = pl.BlockSpec(memory_space=pltpu.VMEM)
SMEM = pl.BlockSpec(memory_space=pltpu.SMEM)


def limit(mib):
    return pltpu.CompilerParams(vmem_limit_bytes=mib * 1024 * 1024)


OFFSETS = tuple(range(-8, 8))
BATCHES = ((0, -1, 1, -2, 2, -3, 3, -4, 4, -5, 5), (-6, 6, -7, 7, -8))
HBM = pl.BlockSpec(memory_space=pltpu.HBM)


def fs_shift(dy, dz):
    return [
        (z * NY + y, ((z + dz) % NZ) * NY + (y + dy) % NY) for z in range(NZ) for y in range(NY)
    ]


def shift(array, dy=0, dz=0):
    return lax.ppermute(array, "fs", fs_shift(dy, dz))


def rolled(array, first_block):
    twice = jnp.concatenate([array, array], axis=1)
    return lax.dynamic_slice_in_dim(twice, first_block * 128, array.shape[1], 1)


def pack_kernel(gate_in, up_in, mix_in, mix_out, down_in, first_ref, second_ref, *scratch):
    held, sems = scratch[:5], scratch[5]
    copies = []
    for k, (src, dst) in enumerate(zip((gate_in, up_in, mix_in, mix_out, down_in), held)):
        copies.append(pltpu.make_async_copy(src, dst, sems.at[k]))
        copies[-1].start()
    for copy in copies:
        copy.wait()
    gate_ref, up_ref, in_ref, out_ref, down_ref = held
    width = gate_ref.shape[1]
    whole = width // 128 * 128
    first_ref[:, :whole] = gate_ref[:, :whole]
    first_ref[:, whole : 2 * whole] = up_ref[:, :whole]
    first_ref[:, 2 * whole :] = jnp.concatenate([gate_ref[:, whole:], up_ref[:, whole:]], axis=1)
    mix = jnp.concatenate([in_ref[...], out_ref[...]], axis=1)
    down_w = down_ref[...]
    rows = [jnp.concatenate([down_w[0:16, :whole], down_w[16:32, :whole]], axis=1)]
    mixed = [mix[8 * g : 8 * g + 8] for g in range(4)]
    mixed += [down_w[8 * g : 8 * g + 8, whole:] for g in range(4)]
    rows.append(jnp.concatenate(mixed, axis=1))
    second_ref[:, 0:SECOND] = jnp.concatenate(rows, axis=0)
    second_ref[:, SECOND:] = jnp.zeros((24, second_ref.shape[1] - SECOND), BF)


def pack(*weights):
    width = 2 * weights[0].shape[1]
    return pl.pallas_call(
        pack_kernel,
        out_shape=(jax.ShapeDtypeStruct((32, width), BF), jax.ShapeDtypeStruct((24, width), BF)),
        in_specs=[HBM] * 5,
        out_specs=(VMEM, VMEM),
        scratch_shapes=[pltpu.VMEM(w.shape, BF) for w in weights] + [pltpu.SemaphoreType.DMA((5,))],
        compiler_params=limit(63),
        cost_estimate=pl.CostEstimate(flops=10**8, bytes_accessed=1 << 18, transcendentals=0),
        name="pack",
    )(*weights)


def by_core(core, blocks):
    even, odd = blocks[0::2], blocks[1::2]
    mine = [jnp.where(core == 0, a, b) for a, b in zip(even, odd)]
    other = [jnp.where(core == 0, b, a) for a, b in zip(even, odd)]
    return jnp.concatenate(mine + other, axis=0)


def first_norm_kernel(at_ref, x_ref, gain_ref, out_ref):
    rows, depth = x_ref.shape
    tile = rows // 8
    block, core = at_ref[0], at_ref[1]
    halves = ([], [])
    for i in range(4):
        x0 = x_ref[2 * i * tile : (2 * i + 1) * tile, :].astype(F32)
        x1 = x_ref[(2 * i + 1) * tile : (2 * i + 2) * tile, :].astype(F32)
        for k, x in enumerate((x0, x1)):
            scale = lax.rsqrt(jnp.mean(x * x, axis=-1, keepdims=True) + 1e-06)
            halves[k].append(scale)
    for p in range(depth // 128):
        start = pl.multiple_of(lax.rem(block + p, depth // 128) * 128, 128)
        gain = gain_ref[0:1, p * 128 : (p + 1) * 128]
        mine, other = [], []
        for i in range(4):
            x0 = x_ref[2 * i * tile : (2 * i + 1) * tile, pl.ds(start, 128)].astype(F32)
            x1 = x_ref[(2 * i + 1) * tile : (2 * i + 2) * tile, pl.ds(start, 128)].astype(F32)
            x0 = (x0 * halves[0][i] * gain).astype(BF)
            x1 = (x1 * halves[1][i] * gain).astype(BF)
            mine.append(jnp.where(core == 0, x0, x1))
            other.append(jnp.where(core == 0, x1, x0))
        for i in range(4):
            out_ref[i * tile : (i + 1) * tile, p * 128 : (p + 1) * 128] = mine[i]
            out_ref[(4 + i) * tile : (5 + i) * tile, p * 128 : (p + 1) * 128] = other[i]


def first_norm(at, tokens, gain):
    return pl.pallas_call(
        first_norm_kernel,
        out_shape=jax.ShapeDtypeStruct(tokens.shape, BF),
        in_specs=[SMEM, VMEM, VMEM],
        out_specs=VMEM,
        compiler_params=limit(8),
        cost_estimate=pl.CostEstimate(flops=10**9, bytes_accessed=3 << 20, transcendentals=0),
        name="first_norm",
    )(at, tokens, gain)


def rms_scale(values, gain):
    return values * lax.rsqrt(jnp.mean(values * values, axis=-1, keepdims=True) + 1e-06) * gain


def settle_kernel(factor, row, parts_ref, stream_ref, gain_ref, new_ref, normed_ref):
    total = parts_ref[0].astype(F32)
    for k in range(1, parts_ref.shape[0]):
        total = total + parts_ref[k].astype(F32)
    stream = stream_ref[...] + factor * rms_scale(total, gain_ref[row : row + 1, :])
    new_ref[...] = stream
    normed = rms_scale(stream, gain_ref[row + 1 : row + 2, :]).astype(BF)
    for k in range(normed_ref.shape[0]):
        normed_ref[k] = normed


def settle(parts, stream, gains, row, factor):
    return pl.pallas_call(
        functools.partial(settle_kernel, factor, row),
        out_shape=(
            jax.ShapeDtypeStruct(stream.shape, F32),
            jax.ShapeDtypeStruct((4, *stream.shape), BF),
        ),
        in_specs=[VMEM] * 3,
        out_specs=(VMEM, VMEM),
        compiler_params=limit(6),
        cost_estimate=pl.CostEstimate(flops=10**8, bytes_accessed=1 << 20, transcendentals=0),
        name="settle",
    )(parts, stream, gains)


def finish_kernel(at_ref, parts_ref, stream_ref, gain_ref, out_ref):
    total = parts_ref[0].astype(F32)
    for k in range(1, parts_ref.shape[0]):
        total = total + parts_ref[k].astype(F32)
    result = (stream_ref[...] + 0.5 * rms_scale(total, gain_ref[5:6, :])).astype(BF)
    blocks = result.shape[1] // 128
    for p in range(blocks):
        start = pl.multiple_of(lax.rem(at_ref[0] + p, blocks) * 128, 128)
        out_ref[:, pl.ds(start, 128)] = result[:, p * 128 : (p + 1) * 128]


def finish(at, parts, stream, gains):
    return pl.pallas_call(
        finish_kernel,
        out_shape=jax.ShapeDtypeStruct(stream.shape, BF),
        in_specs=[SMEM] + [VMEM] * 3,
        out_specs=VMEM,
        compiler_params=limit(6),
        cost_estimate=pl.CostEstimate(flops=10**8, bytes_accessed=1 << 20, transcendentals=0),
        name="finish",
    )(at, parts, stream, gains)


def act(gate, up):
    return (gate / (1.0 + jnp.exp(-gate)) * up).astype(BF)


def gated_product(x, w_ref, out_ref):
    width = out_ref.shape[1]
    whole = width // 128 * 128
    at = 0
    while at < whole:
        n = min(256, whole - at)
        gate = jnp.dot(x, w_ref[:, at : at + n], preferred_element_type=F32)
        up = jnp.dot(x, w_ref[:, whole + at : whole + at + n], preferred_element_type=F32)
        out_ref[:, at : at + n] = act(gate, up)
        at += n
    both = jnp.dot(x, w_ref[:, 2 * whole :], preferred_element_type=F32)
    out_ref[:, whole:] = act(both[:, : width - whole], both[:, width - whole :])


def gated_first_kernel(x_ref, *refs):
    payloads, out_ref, w_ref = refs[:NZ], refs[-2], refs[-1]
    for k in range(NZ):
        w_ref[k * 128 : (k + 1) * 128, :] = payloads[k][0:128, :]
    gated_product(x_ref[...], w_ref, out_ref)


def gated_then_kernel(x_ref, w_ref, out_ref):
    gated_product(x_ref[...], w_ref, out_ref)


def gated(x, weights, width):
    rows, depth = x.shape
    hidden = jax.ShapeDtypeStruct((rows, width), BF)
    whole = jax.ShapeDtypeStruct((depth, 2 * width), BF)
    first = len(weights) > 1
    return pl.pallas_call(
        gated_first_kernel if first else gated_then_kernel,
        out_shape=(hidden, whole) if first else hidden,
        in_specs=[VMEM] * (1 + len(weights)),
        out_specs=(VMEM, VMEM) if first else VMEM,
        compiler_params=limit(16 if first else 10),
        cost_estimate=pl.CostEstimate(
            flops=4 * rows * depth * width, bytes_accessed=8 << 20, transcendentals=0
        ),
        name="gated",
    )(x, *weights)


def absorb_kernel(places, x_ref, *refs):
    n = len(places)
    blocks, total_ref = refs[:n], refs[-1]
    x = [x_ref[:, place * 128 : (place + 1) * 128] for place in places]
    x = x[0] if n == 1 else jnp.concatenate(x, axis=1)
    width = total_ref.shape[1]
    for at in range(0, width, 256):
        end = min(width, at + 256)
        w = [block[0:128, at:end] for block in blocks]
        w = w[0] if n == 1 else jnp.concatenate(w, axis=0)
        part = jnp.dot(x, w, preferred_element_type=F32)
        total_ref[:, at:end] = part if len(refs) == n + 1 else refs[n][:, at:end] + part


def absorb(x, blocks, places, total=None):
    rows, width, n = x.shape[0], blocks[0].shape[1], len(blocks)
    carried = () if total is None else (total,)
    return pl.pallas_call(
        functools.partial(absorb_kernel, places),
        out_shape=jax.ShapeDtypeStruct((rows, width), F32),
        in_specs=[VMEM] * (1 + n + len(carried)),
        out_specs=VMEM,
        input_output_aliases={} if total is None else {1 + n: 0},
        compiler_params=limit(6),
        cost_estimate=pl.CostEstimate(
            flops=2 * rows * width * 128 * n, bytes_accessed=n << 19, transcendentals=0
        ),
        name="absorb",
    )(x, *blocks, *carried)


def silu_kernel(total_ref, mine_ref, other_ref):
    half, width = mine_ref.shape
    whole = width // 128 * 128
    for k, ref in enumerate((mine_ref, other_ref)):
        rows = slice(k * half, (k + 1) * half)
        ref[:, :whole] = act(total_ref[rows, :whole], total_ref[rows, whole : 2 * whole])
        both = total_ref[rows, 2 * whole :]
        ref[:, whole:] = act(both[:, : width - whole], both[:, width - whole :])


def silu(total):
    rows, width = total.shape
    return pl.pallas_call(
        silu_kernel,
        out_shape=(jax.ShapeDtypeStruct((rows // 2, width // 2), BF),) * 2,
        in_specs=[VMEM],
        out_specs=(VMEM, VMEM),
        compiler_params=limit(4),
        cost_estimate=pl.CostEstimate(flops=10**8, bytes_accessed=1 << 20, transcendentals=0),
        name="silu",
    )(total)


def assemble_kernel(y_ref, *refs):
    ins, mix_ref, down_ref = refs[:-2], refs[-2], refs[-1]
    y = y_ref[0]
    whole = SECOND // 2
    for k, batch in enumerate(BATCHES):
        for j in range(NY):
            owner = lax.rem(y - j + NY, NY)
            src = ins[NY * k + j]
            for i, offset in enumerate(batch):
                start = pl.multiple_of(OFFSETS.index(offset) * 128 + owner * 32, 32)
                rows = src[i * 24 : (i + 1) * 24, :]
                wide = [rows[0:16, :whole], rows[0:16, whole:]]
                down_ref[pl.ds(start, 32), 0:whole] = jnp.concatenate(wide, axis=0)
                low = rows[16:24, :]
                mix = [low[:, 256 * g : 256 * g + 256] for g in range(4)]
                mix_ref[pl.ds(start, 32), :] = jnp.concatenate(mix, axis=0)
                rest = [low[:, 1024 + 64 * g : 1088 + 64 * g] for g in range(4)]
                down_ref[pl.ds(start, 32), whole:] = jnp.concatenate(rest, axis=0)


def assemble(y, pieces, down_width):
    rows = NZ * NY * 32
    return pl.pallas_call(
        assemble_kernel,
        out_shape=(
            jax.ShapeDtypeStruct((rows, 256), BF),
            jax.ShapeDtypeStruct((rows, down_width), BF),
        ),
        in_specs=[SMEM] + [VMEM] * len(pieces),
        out_specs=(VMEM, VMEM),
        compiler_params=limit(14),
        cost_estimate=pl.CostEstimate(flops=10**8, bytes_accessed=8 << 20, transcendentals=0),
        name="assemble",
    )(y, *pieces)


def down_kernel(h_ref, w_ref, out_ref):
    h = h_ref[...]
    for at in range(0, w_ref.shape[0], 256):
        out_ref[:, at : at + 256] = lax.dot_general(
            h, w_ref[at : at + 256, :], (((1,), (1,)), ((), ())), preferred_element_type=F32
        ).astype(BF)


def down(hidden, w):
    rows, out = hidden.shape[0], w.shape[0]
    return pl.pallas_call(
        down_kernel,
        out_shape=jax.ShapeDtypeStruct((rows, out), BF),
        in_specs=[VMEM, VMEM],
        out_specs=VMEM,
        compiler_params=limit(14),
        cost_estimate=pl.CostEstimate(
            flops=2 * rows * out * w.shape[1], bytes_accessed=4 << 20, transcendentals=0
        ),
        name="down",
    )(hidden, w)


def pair_kernel(a_ref, b_ref, out_ref):
    rows = out_ref.shape[1]
    for k in range(out_ref.shape[0]):
        at = slice(k * rows, (k + 1) * rows)
        out_ref[k] = (a_ref[at, :].astype(F32) + b_ref[at, :].astype(F32)).astype(BF)


def pair_sum(a, b):
    return pl.pallas_call(
        pair_kernel,
        out_shape=jax.ShapeDtypeStruct((4, a.shape[0] // 4, a.shape[1]), BF),
        in_specs=[VMEM] * 2,
        out_specs=VMEM,
        compiler_params=limit(4),
        cost_estimate=pl.CostEstimate(flops=10**8, bytes_accessed=1 << 20, transcendentals=0),
        name="pair_sum",
    )(a, b)


def mixer_kernel(kind_ref, mine_ref, other_ref, w_ref, pool_ref, scale_ref, keep_ref, send_ref):
    rows = 2 * mine_ref.shape[0]
    tile = rows // 8
    kind, core = kind_ref[0], kind_ref[1]
    x = jnp.concatenate([mine_ref[...], other_ref[...]], axis=0)
    values = jnp.dot(x, w_ref[:, 0:128], preferred_element_type=F32)
    values = values.astype(BF).astype(F32)
    in_order = []
    for i in range(4):
        mine = values[i * tile : (i + 1) * tile]
        other = values[(4 + i) * tile : (5 + i) * tile]
        in_order += [jnp.where(core == 0, mine, other), jnp.where(core == 0, other, mine)]
    values = jnp.concatenate(in_order, axis=0)
    place = lax.broadcasted_iota(jnp.int32, (rows, 128), 0) % LEN
    total = values
    chosen = jnp.zeros_like(values)
    for slot in range(4):
        lag = 2**slot
        earlier = jnp.concatenate([jnp.zeros((lag, 128), F32), total[: rows - lag]], axis=0)
        total = total + jnp.where(place >= lag, earlier, 0.0)
        window = 2 * lag
        mean = total / jnp.minimum(place + 1, window).astype(F32)
        chosen = jnp.where(kind == slot, mean, chosen)
    deviation = (chosen - values).astype(BF)
    mixed = jnp.dot(deviation, pool_ref[...], preferred_element_type=F32)
    mixed = mixed * scale_ref[...].astype(F32)
    mixed = by_core(core, [mixed[i * tile : (i + 1) * tile] for i in range(8)]).astype(BF)
    for at in range(0, w_ref.shape[0], 256):
        share = lax.dot_general(
            mixed, w_ref[at : at + 256, 128:256], (((1,), (1,)), ((), ())), preferred_element_type=F32
        ).astype(BF)
        keep_ref[:, at : at + 256] = share[: rows // 2]
        send_ref[:, at : at + 256] = share[rows // 2 :]


def mixer(kind, mine, other, w, pool_w, pool_scale):
    rows, depth = 2 * mine.shape[0], mine.shape[1]
    return pl.pallas_call(
        mixer_kernel,
        out_shape=(jax.ShapeDtypeStruct((rows // 2, depth), BF),) * 2,
        in_specs=[SMEM] + [VMEM] * 5,
        out_specs=(VMEM, VMEM),
        compiler_params=limit(14),
        cost_estimate=pl.CostEstimate(
            flops=4 * rows * depth * 128, bytes_accessed=4 << 20, transcendentals=0
        ),
        name="mixer",
    )(kind, mine, other, w, pool_w, pool_scale)


X_GROUPS = [[2 * x + core for x in range(4)] for core in range(2)]


def core_swap(array):
    return lax.ppermute(array, "tp", [(k, k ^ 1) for k in range(8)])


def shares_of_rows(mine, other):
    tiles = pair_sum(mine, core_swap(other))
    return lax.all_to_all(tiles, "tp", 0, 0, tiled=True, axis_index_groups=X_GROUPS)


def rows_of_all(copies):
    mine = lax.all_to_all(copies, "tp", 0, 0, tiled=True, axis_index_groups=X_GROUPS)
    mine = mine.reshape(-1, copies.shape[-1])
    return mine, core_swap(mine)


def body(tokens, w_gate, w_up, w_down, w_mix_in, w_mix_out, pool_w, pool_scale, norm_gains):
    tp_size, tp_at = lax.axis_size("tp"), lax.axis_index("tp")
    fs_at = lax.axis_index("fs")
    z, y = fs_at // NY, fs_at % NY
    own_rows = tokens.shape[0] // tp_size
    width = w_gate.shape[1]

    groups = [[k * NY + j for j in range(NY)] for k in range(NZ)]
    first, second = pack(w_gate, w_up, w_mix_in, w_mix_out.T, w_down.T)
    first = lax.all_gather(first, "fs", axis=0, tiled=True, axis_index_groups=groups)

    first_block = lax.rem(z + 8, NZ)
    core = lax.rem(tp_at, 2)
    gains = rolled(norm_gains, first_block)
    numbers = jnp.stack([first_block, core, lax.rem(tp_at, 4), y]).astype(jnp.int32)

    first, late_tokens = lax.optimization_barrier((first, tokens))
    back = ahead = jnp.concatenate([first, second], axis=0)
    x = first_norm(numbers[0:2], late_tokens, gains)
    got = {0: back}
    total = None
    stream = lax.dynamic_slice_in_dim(late_tokens, tp_at * own_rows, own_rows, 0)
    stream = rolled(stream, first_block).astype(F32)
    for k in range(1, 9):
        if k == 7:
            last_second = shift(back[128:, :SECOND], dz=2)
        back = got[-k] = shift(back, dz=1)
        if k < 8:
            ahead = got[k] = shift(ahead, dz=-1)
        places = ([0] if k == 1 else []) + [-k] + ([k] if k < 8 else [])
        total = absorb(x, [got[p] for p in places], tuple(8 + p for p in places), total)
    payloads = [got[k] for k in OFFSETS]

    pieces = []
    for batch in BATCHES:
        own = [last_second if s == -8 else got[s][128:, :SECOND] for s in batch]
        own = jnp.concatenate(own, axis=0)
        pieces += [own, shift(own, dy=1), shift(own, dy=2), shift(own, dy=-1)]
    mix_w, down_w = assemble(numbers[3:4], pieces, width)

    hidden, other = silu(total)
    other, mine = down(other, down_w), down(hidden, down_w)
    parts = shares_of_rows(mine, other)
    stream, copies = settle(parts, stream, gains, 1, 0.5)
    kind = jnp.stack([numbers[2], numbers[1]])
    share = mixer(kind, *rows_of_all(copies), mix_w, pool_w[0], pool_scale[None])
    stream, copies = settle(shares_of_rows(*share), stream, gains, 3, 1.0)
    mine, other = rows_of_all(copies)
    hidden, gate_up = gated(mine, payloads, width)
    other = gated(other, [gate_up], width)
    other, mine = down(other, down_w), down(hidden, down_w)
    parts = shares_of_rows(mine, other)
    return finish(numbers[0:1], parts, stream, gains)


def solution(mesh):
    in_specs = (
        P("fs", None),
        P("fs", "tp"),
        P("fs", "tp"),
        P("tp", "fs"),
        P("fs", "tp"),
        P("tp", "fs"),
        P("tp", None, None),
        P("tp"),
        P(),
    )
    out_specs = P(("fs", "tp"), None)

    return jax.shard_map(body, mesh=mesh, in_specs=in_specs, out_specs=out_specs, check_vma=False)
```

```python
import functools

import jax
import jax.numpy as jnp
from jax import lax
from jax.experimental import pallas as pl
from jax.experimental.pallas import tpu as pltpu
from jax.sharding import PartitionSpec as P


LEN = 64
NZ, NY = 16, 4
BF = jnp.bfloat16
F32 = jnp.float32
VMEM = pl.BlockSpec(memory_space=pltpu.VMEM)
SMEM = pl.BlockSpec(memory_space=pltpu.SMEM)


def limit(mib):
    return pltpu.CompilerParams(vmem_limit_bytes=mib * 1024 * 1024)


OFFSETS = tuple(range(-8, 8))
BATCHES = ((0, -1, 1, -2, 2, -3, 3, -4, 4, -5, 5), (-6, 6, -7, 7, -8))
HBM = pl.BlockSpec(memory_space=pltpu.HBM)


def fs_shift(dy, dz):
    return [
        (z * NY + y, ((z + dz) % NZ) * NY + (y + dy) % NY) for z in range(NZ) for y in range(NY)
    ]


def shift(array, dy=0, dz=0):
    return lax.ppermute(array, "fs", fs_shift(dy, dz))


def rolled(array, first_block):
    twice = jnp.concatenate([array, array], axis=1)
    return lax.dynamic_slice_in_dim(twice, first_block * 128, array.shape[1], 1)


def pack_kernel(gate_in, up_in, mix_in, mix_out, down_in, first_ref, second_ref, *scratch):
    held, sems = scratch[:5], scratch[5]
    copies = []
    for k, (src, dst) in enumerate(zip((gate_in, up_in, mix_in, mix_out, down_in), held)):
        copies.append(pltpu.make_async_copy(src, dst, sems.at[k]))
        copies[-1].start()
    for copy in copies:
        copy.wait()
    gate_ref, up_ref, in_ref, out_ref, down_ref = held
    width = gate_ref.shape[1]
    whole = width // 128 * 128
    first_ref[:, :whole] = gate_ref[:, :whole]
    first_ref[:, whole : 2 * whole] = up_ref[:, :whole]
    first_ref[:, 2 * whole :] = jnp.concatenate([gate_ref[:, whole:], up_ref[:, whole:]], axis=1)
    second_ref[:, 0:128] = in_ref[...]
    second_ref[:, 128:256] = out_ref[...]
    second_ref[:, 256 : 256 + width] = down_ref[...]
    second_ref[:, 256 + width :] = jnp.zeros((32, width - 256), BF)


def pack(*weights):
    shape = jax.ShapeDtypeStruct((32, 2 * weights[0].shape[1]), BF)
    return pl.pallas_call(
        pack_kernel,
        out_shape=(shape, shape),
        in_specs=[HBM] * 5,
        out_specs=(VMEM, VMEM),
        scratch_shapes=[pltpu.VMEM(w.shape, BF) for w in weights] + [pltpu.SemaphoreType.DMA((5,))],
        compiler_params=limit(63),
        cost_estimate=pl.CostEstimate(flops=10**8, bytes_accessed=1 << 18, transcendentals=0),
        name="pack",
    )(*weights)


def by_core(core, blocks):
    even, odd = blocks[0::2], blocks[1::2]
    mine = [jnp.where(core == 0, a, b) for a, b in zip(even, odd)]
    other = [jnp.where(core == 0, b, a) for a, b in zip(even, odd)]
    return jnp.concatenate(mine + other, axis=0)


def first_norm_kernel(at_ref, x_ref, gain_ref, out_ref):
    rows, depth = x_ref.shape
    tile = rows // 8
    block, core = at_ref[0], at_ref[1]
    halves = ([], [])
    for i in range(4):
        x0 = x_ref[2 * i * tile : (2 * i + 1) * tile, :].astype(F32)
        x1 = x_ref[(2 * i + 1) * tile : (2 * i + 2) * tile, :].astype(F32)
        for k, x in enumerate((x0, x1)):
            scale = lax.rsqrt(jnp.mean(x * x, axis=-1, keepdims=True) + 1e-06)
            halves[k].append(scale)
    for p in range(depth // 128):
        start = pl.multiple_of(lax.rem(block + p, depth // 128) * 128, 128)
        gain = gain_ref[0:1, p * 128 : (p + 1) * 128]
        mine, other = [], []
        for i in range(4):
            x0 = x_ref[2 * i * tile : (2 * i + 1) * tile, pl.ds(start, 128)].astype(F32)
            x1 = x_ref[(2 * i + 1) * tile : (2 * i + 2) * tile, pl.ds(start, 128)].astype(F32)
            x0 = (x0 * halves[0][i] * gain).astype(BF)
            x1 = (x1 * halves[1][i] * gain).astype(BF)
            mine.append(jnp.where(core == 0, x0, x1))
            other.append(jnp.where(core == 0, x1, x0))
        for i in range(4):
            out_ref[i * tile : (i + 1) * tile, p * 128 : (p + 1) * 128] = mine[i]
            out_ref[(4 + i) * tile : (5 + i) * tile, p * 128 : (p + 1) * 128] = other[i]


def first_norm(at, tokens, gain):
    return pl.pallas_call(
        first_norm_kernel,
        out_shape=jax.ShapeDtypeStruct(tokens.shape, BF),
        in_specs=[SMEM, VMEM, VMEM],
        out_specs=VMEM,
        compiler_params=limit(8),
        cost_estimate=pl.CostEstimate(flops=10**9, bytes_accessed=3 << 20, transcendentals=0),
        name="first_norm",
    )(at, tokens, gain)


def rms_scale(values, gain):
    return values * lax.rsqrt(jnp.mean(values * values, axis=-1, keepdims=True) + 1e-06) * gain


def settle_kernel(factor, row, parts_ref, stream_ref, gain_ref, new_ref, normed_ref):
    total = parts_ref[0].astype(F32)
    for k in range(1, parts_ref.shape[0]):
        total = total + parts_ref[k].astype(F32)
    stream = stream_ref[...] + factor * rms_scale(total, gain_ref[row : row + 1, :])
    new_ref[...] = stream
    normed = rms_scale(stream, gain_ref[row + 1 : row + 2, :]).astype(BF)
    for k in range(normed_ref.shape[0]):
        normed_ref[k] = normed


def settle(parts, stream, gains, row, factor):
    return pl.pallas_call(
        functools.partial(settle_kernel, factor, row),
        out_shape=(
            jax.ShapeDtypeStruct(stream.shape, F32),
            jax.ShapeDtypeStruct((4, *stream.shape), BF),
        ),
        in_specs=[VMEM] * 3,
        out_specs=(VMEM, VMEM),
        compiler_params=limit(6),
        cost_estimate=pl.CostEstimate(flops=10**8, bytes_accessed=1 << 20, transcendentals=0),
        name="settle",
    )(parts, stream, gains)


def finish_kernel(at_ref, parts_ref, stream_ref, gain_ref, out_ref):
    total = parts_ref[0].astype(F32)
    for k in range(1, parts_ref.shape[0]):
        total = total + parts_ref[k].astype(F32)
    result = (stream_ref[...] + 0.5 * rms_scale(total, gain_ref[5:6, :])).astype(BF)
    blocks = result.shape[1] // 128
    for p in range(blocks):
        start = pl.multiple_of(lax.rem(at_ref[0] + p, blocks) * 128, 128)
        out_ref[:, pl.ds(start, 128)] = result[:, p * 128 : (p + 1) * 128]


def finish(at, parts, stream, gains):
    return pl.pallas_call(
        finish_kernel,
        out_shape=jax.ShapeDtypeStruct(stream.shape, BF),
        in_specs=[SMEM] + [VMEM] * 3,
        out_specs=VMEM,
        compiler_params=limit(6),
        cost_estimate=pl.CostEstimate(flops=10**8, bytes_accessed=1 << 20, transcendentals=0),
        name="finish",
    )(at, parts, stream, gains)


def act(gate, up):
    return (gate / (1.0 + jnp.exp(-gate)) * up).astype(BF)


def gated_product(x, w_ref, out_ref):
    width = out_ref.shape[1]
    whole = width // 128 * 128
    at = 0
    while at < whole:
        n = min(256, whole - at)
        gate = jnp.dot(x, w_ref[:, at : at + n], preferred_element_type=F32)
        up = jnp.dot(x, w_ref[:, whole + at : whole + at + n], preferred_element_type=F32)
        out_ref[:, at : at + n] = act(gate, up)
        at += n
    both = jnp.dot(x, w_ref[:, 2 * whole :], preferred_element_type=F32)
    out_ref[:, whole:] = act(both[:, : width - whole], both[:, width - whole :])


def gated_first_kernel(x_ref, *refs):
    payloads, out_ref, w_ref = refs[:NZ], refs[-2], refs[-1]
    for k in range(NZ):
        w_ref[k * 128 : (k + 1) * 128, :] = payloads[k][0:128, :]
    gated_product(x_ref[...], w_ref, out_ref)


def gated_then_kernel(x_ref, w_ref, out_ref):
    gated_product(x_ref[...], w_ref, out_ref)


def gated(x, weights, width):
    rows, depth = x.shape
    hidden = jax.ShapeDtypeStruct((rows, width), BF)
    whole = jax.ShapeDtypeStruct((depth, 2 * width), BF)
    first = len(weights) > 1
    return pl.pallas_call(
        gated_first_kernel if first else gated_then_kernel,
        out_shape=(hidden, whole) if first else hidden,
        in_specs=[VMEM] * (1 + len(weights)),
        out_specs=(VMEM, VMEM) if first else VMEM,
        compiler_params=limit(16 if first else 10),
        cost_estimate=pl.CostEstimate(
            flops=4 * rows * depth * width, bytes_accessed=8 << 20, transcendentals=0
        ),
        name="gated",
    )(x, *weights)


def absorb_kernel(places, x_ref, *refs):
    n = len(places)
    blocks, total_ref = refs[:n], refs[-1]
    x = [x_ref[:, place * 128 : (place + 1) * 128] for place in places]
    x = x[0] if n == 1 else jnp.concatenate(x, axis=1)
    width = total_ref.shape[1]
    for at in range(0, width, 256):
        end = min(width, at + 256)
        w = [block[0:128, at:end] for block in blocks]
        w = w[0] if n == 1 else jnp.concatenate(w, axis=0)
        part = jnp.dot(x, w, preferred_element_type=F32)
        total_ref[:, at:end] = part if len(refs) == n + 1 else refs[n][:, at:end] + part


def absorb(x, blocks, places, total=None):
    rows, width, n = x.shape[0], blocks[0].shape[1], len(blocks)
    carried = () if total is None else (total,)
    return pl.pallas_call(
        functools.partial(absorb_kernel, places),
        out_shape=jax.ShapeDtypeStruct((rows, width), F32),
        in_specs=[VMEM] * (1 + n + len(carried)),
        out_specs=VMEM,
        input_output_aliases={} if total is None else {1 + n: 0},
        compiler_params=limit(6),
        cost_estimate=pl.CostEstimate(
            flops=2 * rows * width * 128 * n, bytes_accessed=n << 19, transcendentals=0
        ),
        name="absorb",
    )(x, *blocks, *carried)


def silu_kernel(total_ref, mine_ref, other_ref):
    half, width = mine_ref.shape
    whole = width // 128 * 128
    for k, ref in enumerate((mine_ref, other_ref)):
        rows = slice(k * half, (k + 1) * half)
        ref[:, :whole] = act(total_ref[rows, :whole], total_ref[rows, whole : 2 * whole])
        both = total_ref[rows, 2 * whole :]
        ref[:, whole:] = act(both[:, : width - whole], both[:, width - whole :])


def silu(total):
    rows, width = total.shape
    return pl.pallas_call(
        silu_kernel,
        out_shape=(jax.ShapeDtypeStruct((rows // 2, width // 2), BF),) * 2,
        in_specs=[VMEM],
        out_specs=(VMEM, VMEM),
        compiler_params=limit(4),
        cost_estimate=pl.CostEstimate(flops=10**8, bytes_accessed=1 << 20, transcendentals=0),
        name="silu",
    )(total)


def assemble_kernel(y_ref, *refs):
    ins, mix_ref, down_ref = refs[:-2], refs[-2], refs[-1]
    y = y_ref[0]
    width = mix_ref.shape[1] + down_ref.shape[1]
    for k, batch in enumerate(BATCHES):
        for j in range(NY):
            owner = lax.rem(y - j + NY, NY)
            src = ins[NY * k + j]
            for i, offset in enumerate(batch):
                start = pl.multiple_of(OFFSETS.index(offset) * 128 + owner * 32, 32)
                mix_ref[pl.ds(start, 32), :] = src[i * 32 : (i + 1) * 32, 0:256]
                down_ref[pl.ds(start, 32), :] = src[i * 32 : (i + 1) * 32, 256:width]


def assemble(y, pieces, down_width):
    rows = NZ * NY * 32
    return pl.pallas_call(
        assemble_kernel,
        out_shape=(
            jax.ShapeDtypeStruct((rows, 256), BF),
            jax.ShapeDtypeStruct((rows, down_width), BF),
        ),
        in_specs=[SMEM] + [VMEM] * len(pieces),
        out_specs=(VMEM, VMEM),
        compiler_params=limit(14),
        cost_estimate=pl.CostEstimate(flops=10**8, bytes_accessed=8 << 20, transcendentals=0),
        name="assemble",
    )(y, *pieces)


def down_kernel(h_ref, w_ref, out_ref):
    h = h_ref[...]
    for at in range(0, w_ref.shape[0], 256):
        out_ref[:, at : at + 256] = lax.dot_general(
            h, w_ref[at : at + 256, :], (((1,), (1,)), ((), ())), preferred_element_type=F32
        ).astype(BF)


def down(hidden, w):
    rows, out = hidden.shape[0], w.shape[0]
    return pl.pallas_call(
        down_kernel,
        out_shape=jax.ShapeDtypeStruct((rows, out), BF),
        in_specs=[VMEM, VMEM],
        out_specs=VMEM,
        compiler_params=limit(14),
        cost_estimate=pl.CostEstimate(
            flops=2 * rows * out * w.shape[1], bytes_accessed=4 << 20, transcendentals=0
        ),
        name="down",
    )(hidden, w)


def pair_kernel(a_ref, b_ref, out_ref):
    rows = out_ref.shape[1]
    for k in range(out_ref.shape[0]):
        at = slice(k * rows, (k + 1) * rows)
        out_ref[k] = (a_ref[at, :].astype(F32) + b_ref[at, :].astype(F32)).astype(BF)


def pair_sum(a, b):
    return pl.pallas_call(
        pair_kernel,
        out_shape=jax.ShapeDtypeStruct((4, a.shape[0] // 4, a.shape[1]), BF),
        in_specs=[VMEM] * 2,
        out_specs=VMEM,
        compiler_params=limit(4),
        cost_estimate=pl.CostEstimate(flops=10**8, bytes_accessed=1 << 20, transcendentals=0),
        name="pair_sum",
    )(a, b)


def mixer_kernel(kind_ref, mine_ref, other_ref, w_ref, pool_ref, scale_ref, keep_ref, send_ref):
    rows = 2 * mine_ref.shape[0]
    tile = rows // 8
    kind, core = kind_ref[0], kind_ref[1]
    x = jnp.concatenate([mine_ref[...], other_ref[...]], axis=0)
    values = jnp.dot(x, w_ref[:, 0:128], preferred_element_type=F32)
    values = values.astype(BF).astype(F32)
    in_order = []
    for i in range(4):
        mine = values[i * tile : (i + 1) * tile]
        other = values[(4 + i) * tile : (5 + i) * tile]
        in_order += [jnp.where(core == 0, mine, other), jnp.where(core == 0, other, mine)]
    values = jnp.concatenate(in_order, axis=0)
    place = lax.broadcasted_iota(jnp.int32, (rows, 128), 0) % LEN
    total = values
    chosen = jnp.zeros_like(values)
    for slot in range(4):
        lag = 2**slot
        earlier = jnp.concatenate([jnp.zeros((lag, 128), F32), total[: rows - lag]], axis=0)
        total = total + jnp.where(place >= lag, earlier, 0.0)
        window = 2 * lag
        mean = total / jnp.minimum(place + 1, window).astype(F32)
        chosen = jnp.where(kind == slot, mean, chosen)
    deviation = (chosen - values).astype(BF)
    mixed = jnp.dot(deviation, pool_ref[...], preferred_element_type=F32)
    mixed = mixed * scale_ref[...].astype(F32)
    mixed = by_core(core, [mixed[i * tile : (i + 1) * tile] for i in range(8)]).astype(BF)
    for at in range(0, w_ref.shape[0], 256):
        share = lax.dot_general(
            mixed, w_ref[at : at + 256, 128:256], (((1,), (1,)), ((), ())), preferred_element_type=F32
        ).astype(BF)
        keep_ref[:, at : at + 256] = share[: rows // 2]
        send_ref[:, at : at + 256] = share[rows // 2 :]


def mixer(kind, mine, other, w, pool_w, pool_scale):
    rows, depth = 2 * mine.shape[0], mine.shape[1]
    return pl.pallas_call(
        mixer_kernel,
        out_shape=(jax.ShapeDtypeStruct((rows // 2, depth), BF),) * 2,
        in_specs=[SMEM] + [VMEM] * 5,
        out_specs=(VMEM, VMEM),
        compiler_params=limit(14),
        cost_estimate=pl.CostEstimate(
            flops=4 * rows * depth * 128, bytes_accessed=4 << 20, transcendentals=0
        ),
        name="mixer",
    )(kind, mine, other, w, pool_w, pool_scale)


X_GROUPS = [[2 * x + core for x in range(4)] for core in range(2)]


def core_swap(array):
    return lax.ppermute(array, "tp", [(k, k ^ 1) for k in range(8)])


def shares_of_rows(mine, other):
    tiles = pair_sum(mine, core_swap(other))
    return lax.all_to_all(tiles, "tp", 0, 0, tiled=True, axis_index_groups=X_GROUPS)


def rows_of_all(copies):
    mine = lax.all_to_all(copies, "tp", 0, 0, tiled=True, axis_index_groups=X_GROUPS)
    mine = mine.reshape(-1, copies.shape[-1])
    return mine, core_swap(mine)


def body(tokens, w_gate, w_up, w_down, w_mix_in, w_mix_out, pool_w, pool_scale, norm_gains):
    tp_size, tp_at = lax.axis_size("tp"), lax.axis_index("tp")
    fs_at = lax.axis_index("fs")
    z, y = fs_at // NY, fs_at % NY
    own_rows = tokens.shape[0] // tp_size
    width = w_gate.shape[1]

    groups = [[k * NY + j for j in range(NY)] for k in range(NZ)]
    second_width = 256 + width
    first, second = pack(w_gate, w_up, w_mix_in, w_mix_out.T, w_down.T)
    first = lax.all_gather(first, "fs", axis=0, tiled=True, axis_index_groups=groups)

    first_block = lax.rem(z + 8, NZ)
    core = lax.rem(tp_at, 2)
    gains = rolled(norm_gains, first_block)
    numbers = jnp.stack([first_block, core, lax.rem(tp_at, 4), y]).astype(jnp.int32)

    first, late_tokens = lax.optimization_barrier((first, tokens))
    back = ahead = jnp.concatenate([first, second], axis=0)
    x = first_norm(numbers[0:2], late_tokens, gains)
    got = {0: back}
    total = None
    for k in range(1, 9):
        if k == 7:
            last_second = shift(back[128:, :second_width], dz=2)
        back = got[-k] = shift(back, dz=1)
        if k < 8:
            ahead = got[k] = shift(ahead, dz=-1)
        places = ([0] if k == 1 else []) + [-k] + ([k] if k < 8 else [])
        total = absorb(x, [got[p] for p in places], tuple(8 + p for p in places), total)
    payloads = [got[k] for k in OFFSETS]

    pieces = []
    for batch in BATCHES:
        own = [last_second if s == -8 else got[s][128:, :second_width] for s in batch]
        own = jnp.concatenate(own, axis=0)
        pieces += [own, shift(own, dy=1), shift(own, dy=2), shift(own, dy=-1)]
    mix_w, down_w = assemble(numbers[3:4], pieces, width)

    stream = lax.dynamic_slice_in_dim(late_tokens, tp_at * own_rows, own_rows, 0)
    stream = rolled(stream, first_block).astype(F32)
    hidden, other = silu(total)
    other, mine = down(other, down_w), down(hidden, down_w)
    parts = shares_of_rows(mine, other)
    stream, copies = settle(parts, stream, gains, 1, 0.5)
    kind = jnp.stack([numbers[2], numbers[1]])
    share = mixer(kind, *rows_of_all(copies), mix_w, pool_w[0], pool_scale[None])
    stream, copies = settle(shares_of_rows(*share), stream, gains, 3, 1.0)
    mine, other = rows_of_all(copies)
    hidden, gate_up = gated(mine, payloads, width)
    other = gated(other, [gate_up], width)
    other, mine = down(other, down_w), down(hidden, down_w)
    parts = shares_of_rows(mine, other)
    return finish(numbers[0:1], parts, stream, gains)


def solution(mesh):
    in_specs = (
        P("fs", None),
        P("fs", "tp"),
        P("fs", "tp"),
        P("tp", "fs"),
        P("fs", "tp"),
        P("tp", "fs"),
        P("tp", None, None),
        P("tp"),
        P(),
    )
    out_specs = P(("fs", "tp"), None)

    return jax.shard_map(body, mesh=mesh, in_specs=in_specs, out_specs=out_specs, check_vma=False)
```

```python
import functools

import jax
import jax.numpy as jnp
from jax import lax
from jax.experimental import pallas as pl
from jax.experimental.pallas import tpu as pltpu
from jax.sharding import PartitionSpec as P


LEN = 64
NZ, NY = 16, 4
BF = jnp.bfloat16
F32 = jnp.float32
VMEM = pl.BlockSpec(memory_space=pltpu.VMEM)
SMEM = pl.BlockSpec(memory_space=pltpu.SMEM)


def limit(mib):
    return pltpu.CompilerParams(vmem_limit_bytes=mib * 1024 * 1024)


OFFSETS = tuple(range(-8, 8))
BATCHES = ((0, -1, 1, -2, 2, -3, 3, -4, 4, -5, 5), (-6, 6, -7, 7, -8))
HBM = pl.BlockSpec(memory_space=pltpu.HBM)


def fs_shift(dy, dz):
    return [
        (z * NY + y, ((z + dz) % NZ) * NY + (y + dy) % NY) for z in range(NZ) for y in range(NY)
    ]


def shift(array, dy=0, dz=0):
    return lax.ppermute(array, "fs", fs_shift(dy, dz))


def rolled(array, first_block):
    twice = jnp.concatenate([array, array], axis=1)
    return lax.dynamic_slice_in_dim(twice, first_block * 128, array.shape[1], 1)


def pack_kernel(gate_in, up_in, mix_in, mix_out, down_in, first_ref, second_ref, *scratch):
    held, sems = scratch[:5], scratch[5]
    copies = []
    for k, (src, dst) in enumerate(zip((gate_in, up_in, mix_in, mix_out, down_in), held)):
        copies.append(pltpu.make_async_copy(src, dst, sems.at[k]))
        copies[-1].start()
    for copy in copies:
        copy.wait()
    gate_ref, up_ref, in_ref, out_ref, down_ref = held
    width = gate_ref.shape[1]
    whole = width // 128 * 128
    first_ref[:, :whole] = gate_ref[:, :whole]
    first_ref[:, whole : 2 * whole] = up_ref[:, :whole]
    first_ref[:, 2 * whole :] = jnp.concatenate([gate_ref[:, whole:], up_ref[:, whole:]], axis=1)
    second_ref[:, 0:128] = in_ref[...]
    second_ref[:, 128:256] = out_ref[...]
    second_ref[:, 256 : 256 + width] = down_ref[...]
    second_ref[:, 256 + width :] = jnp.zeros((32, width - 256), BF)


def pack(*weights):
    shape = jax.ShapeDtypeStruct((32, 2 * weights[0].shape[1]), BF)
    return pl.pallas_call(
        pack_kernel,
        out_shape=(shape, shape),
        in_specs=[HBM] * 5,
        out_specs=(VMEM, VMEM),
        scratch_shapes=[pltpu.VMEM(w.shape, BF) for w in weights] + [pltpu.SemaphoreType.DMA((5,))],
        compiler_params=limit(63),
        cost_estimate=pl.CostEstimate(flops=10**8, bytes_accessed=1 << 18, transcendentals=0),
        name="pack",
    )(*weights)


def by_core(core, blocks):
    even, odd = blocks[0::2], blocks[1::2]
    mine = [jnp.where(core == 0, a, b) for a, b in zip(even, odd)]
    other = [jnp.where(core == 0, b, a) for a, b in zip(even, odd)]
    return jnp.concatenate(mine + other, axis=0)


def first_norm_kernel(at_ref, x_ref, gain_ref, out_ref):
    rows, depth = x_ref.shape
    tile = rows // 8
    block, core = at_ref[0], at_ref[1]
    halves = ([], [])
    for i in range(4):
        x0 = x_ref[2 * i * tile : (2 * i + 1) * tile, :].astype(F32)
        x1 = x_ref[(2 * i + 1) * tile : (2 * i + 2) * tile, :].astype(F32)
        for k, x in enumerate((x0, x1)):
            scale = lax.rsqrt(jnp.mean(x * x, axis=-1, keepdims=True) + 1e-06)
            halves[k].append(scale)
    for p in range(depth // 128):
        start = pl.multiple_of(lax.rem(block + p, depth // 128) * 128, 128)
        gain = gain_ref[0:1, p * 128 : (p + 1) * 128]
        mine, other = [], []
        for i in range(4):
            x0 = x_ref[2 * i * tile : (2 * i + 1) * tile, pl.ds(start, 128)].astype(F32)
            x1 = x_ref[(2 * i + 1) * tile : (2 * i + 2) * tile, pl.ds(start, 128)].astype(F32)
            x0 = (x0 * halves[0][i] * gain).astype(BF)
            x1 = (x1 * halves[1][i] * gain).astype(BF)
            mine.append(jnp.where(core == 0, x0, x1))
            other.append(jnp.where(core == 0, x1, x0))
        for i in range(4):
            out_ref[i * tile : (i + 1) * tile, p * 128 : (p + 1) * 128] = mine[i]
            out_ref[(4 + i) * tile : (5 + i) * tile, p * 128 : (p + 1) * 128] = other[i]


def first_norm(at, tokens, gain):
    return pl.pallas_call(
        first_norm_kernel,
        out_shape=jax.ShapeDtypeStruct(tokens.shape, BF),
        in_specs=[SMEM, VMEM, VMEM],
        out_specs=VMEM,
        compiler_params=limit(8),
        cost_estimate=pl.CostEstimate(flops=10**9, bytes_accessed=3 << 20, transcendentals=0),
        name="first_norm",
    )(at, tokens, gain)


def rms_scale(values, gain):
    return values * lax.rsqrt(jnp.mean(values * values, axis=-1, keepdims=True) + 1e-06) * gain


def settle_kernel(factor, row, parts_ref, stream_ref, gain_ref, new_ref, normed_ref):
    total = parts_ref[0].astype(F32)
    for k in range(1, parts_ref.shape[0]):
        total = total + parts_ref[k].astype(F32)
    stream = stream_ref[...] + factor * rms_scale(total, gain_ref[row : row + 1, :])
    new_ref[...] = stream
    normed = rms_scale(stream, gain_ref[row + 1 : row + 2, :]).astype(BF)
    for k in range(normed_ref.shape[0]):
        normed_ref[k] = normed


def settle(parts, stream, gains, row, factor):
    return pl.pallas_call(
        functools.partial(settle_kernel, factor, row),
        out_shape=(
            jax.ShapeDtypeStruct(stream.shape, F32),
            jax.ShapeDtypeStruct((4, *stream.shape), BF),
        ),
        in_specs=[VMEM] * 3,
        out_specs=(VMEM, VMEM),
        compiler_params=limit(6),
        cost_estimate=pl.CostEstimate(flops=10**8, bytes_accessed=1 << 20, transcendentals=0),
        name="settle",
    )(parts, stream, gains)


def finish_kernel(at_ref, parts_ref, stream_ref, gain_ref, out_ref):
    total = parts_ref[0].astype(F32)
    for k in range(1, parts_ref.shape[0]):
        total = total + parts_ref[k].astype(F32)
    result = (stream_ref[...] + 0.5 * rms_scale(total, gain_ref[5:6, :])).astype(BF)
    blocks = result.shape[1] // 128
    for p in range(blocks):
        start = pl.multiple_of(lax.rem(at_ref[0] + p, blocks) * 128, 128)
        out_ref[:, pl.ds(start, 128)] = result[:, p * 128 : (p + 1) * 128]


def finish(at, parts, stream, gains):
    return pl.pallas_call(
        finish_kernel,
        out_shape=jax.ShapeDtypeStruct(stream.shape, BF),
        in_specs=[SMEM] + [VMEM] * 3,
        out_specs=VMEM,
        compiler_params=limit(6),
        cost_estimate=pl.CostEstimate(flops=10**8, bytes_accessed=1 << 20, transcendentals=0),
        name="finish",
    )(at, parts, stream, gains)


def act(gate, up):
    return (gate / (1.0 + jnp.exp(-gate)) * up).astype(BF)


def gated_product(x, w_ref, out_ref):
    width = out_ref.shape[1]
    whole = width // 128 * 128
    at = 0
    while at < whole:
        n = min(256, whole - at)
        gate = jnp.dot(x, w_ref[:, at : at + n], preferred_element_type=F32)
        up = jnp.dot(x, w_ref[:, whole + at : whole + at + n], preferred_element_type=F32)
        out_ref[:, at : at + n] = act(gate, up)
        at += n
    both = jnp.dot(x, w_ref[:, 2 * whole :], preferred_element_type=F32)
    out_ref[:, whole:] = act(both[:, : width - whole], both[:, width - whole :])


def gated_first_kernel(x_ref, *refs):
    payloads, out_ref, w_ref = refs[:NZ], refs[-2], refs[-1]
    for k in range(NZ):
        w_ref[k * 128 : (k + 1) * 128, :] = payloads[k][0:128, :]
    gated_product(x_ref[...], w_ref, out_ref)


def gated_then_kernel(x_ref, w_ref, out_ref):
    gated_product(x_ref[...], w_ref, out_ref)


def gated(x, weights, width):
    rows, depth = x.shape
    hidden = jax.ShapeDtypeStruct((rows, width), BF)
    whole = jax.ShapeDtypeStruct((depth, 2 * width), BF)
    first = len(weights) > 1
    return pl.pallas_call(
        gated_first_kernel if first else gated_then_kernel,
        out_shape=(hidden, whole) if first else hidden,
        in_specs=[VMEM] * (1 + len(weights)),
        out_specs=(VMEM, VMEM) if first else VMEM,
        compiler_params=limit(16 if first else 10),
        cost_estimate=pl.CostEstimate(
            flops=4 * rows * depth * width, bytes_accessed=8 << 20, transcendentals=0
        ),
        name="gated",
    )(x, *weights)


def absorb_kernel(places, x_ref, *refs):
    n = len(places)
    blocks, total_ref = refs[:n], refs[-1]
    x = [x_ref[:, place * 128 : (place + 1) * 128] for place in places]
    x = x[0] if n == 1 else jnp.concatenate(x, axis=1)
    width = total_ref.shape[1]
    for at in range(0, width, 256):
        end = min(width, at + 256)
        w = [block[0:128, at:end] for block in blocks]
        w = w[0] if n == 1 else jnp.concatenate(w, axis=0)
        part = jnp.dot(x, w, preferred_element_type=F32)
        total_ref[:, at:end] = part if len(refs) == n + 1 else refs[n][:, at:end] + part


def absorb(x, blocks, places, total=None):
    rows, width, n = x.shape[0], blocks[0].shape[1], len(blocks)
    carried = () if total is None else (total,)
    return pl.pallas_call(
        functools.partial(absorb_kernel, places),
        out_shape=jax.ShapeDtypeStruct((rows, width), F32),
        in_specs=[VMEM] * (1 + n + len(carried)),
        out_specs=VMEM,
        input_output_aliases={} if total is None else {1 + n: 0},
        compiler_params=limit(6),
        cost_estimate=pl.CostEstimate(
            flops=2 * rows * width * 128 * n, bytes_accessed=n << 19, transcendentals=0
        ),
        name="absorb",
    )(x, *blocks, *carried)


def silu_kernel(total_ref, mine_ref, other_ref):
    half, width = mine_ref.shape
    whole = width // 128 * 128
    for k, ref in enumerate((mine_ref, other_ref)):
        rows = slice(k * half, (k + 1) * half)
        ref[:, :whole] = act(total_ref[rows, :whole], total_ref[rows, whole : 2 * whole])
        both = total_ref[rows, 2 * whole :]
        ref[:, whole:] = act(both[:, : width - whole], both[:, width - whole :])


def silu(total):
    rows, width = total.shape
    return pl.pallas_call(
        silu_kernel,
        out_shape=(jax.ShapeDtypeStruct((rows // 2, width // 2), BF),) * 2,
        in_specs=[VMEM],
        out_specs=(VMEM, VMEM),
        compiler_params=limit(4),
        cost_estimate=pl.CostEstimate(flops=10**8, bytes_accessed=1 << 20, transcendentals=0),
        name="silu",
    )(total)


def assemble_kernel(y_ref, *refs):
    ins, mix_ref, down_ref = refs[:-2], refs[-2], refs[-1]
    y = y_ref[0]
    width = mix_ref.shape[1] + down_ref.shape[1]
    for k, batch in enumerate(BATCHES):
        for j in range(NY):
            owner = lax.rem(y - j + NY, NY)
            src = ins[NY * k + j]
            for i, offset in enumerate(batch):
                start = pl.multiple_of(OFFSETS.index(offset) * 128 + owner * 32, 32)
                mix_ref[pl.ds(start, 32), :] = src[i * 32 : (i + 1) * 32, 0:256]
                down_ref[pl.ds(start, 32), :] = src[i * 32 : (i + 1) * 32, 256:width]


def assemble(y, pieces, down_width):
    rows = NZ * NY * 32
    return pl.pallas_call(
        assemble_kernel,
        out_shape=(
            jax.ShapeDtypeStruct((rows, 256), BF),
            jax.ShapeDtypeStruct((rows, down_width), BF),
        ),
        in_specs=[SMEM] + [VMEM] * len(pieces),
        out_specs=(VMEM, VMEM),
        compiler_params=limit(14),
        cost_estimate=pl.CostEstimate(flops=10**8, bytes_accessed=8 << 20, transcendentals=0),
        name="assemble",
    )(y, *pieces)


def down_kernel(h_ref, w_ref, out_ref):
    h = h_ref[...]
    for at in range(0, w_ref.shape[0], 256):
        out_ref[:, at : at + 256] = lax.dot_general(
            h, w_ref[at : at + 256, :], (((1,), (1,)), ((), ())), preferred_element_type=F32
        ).astype(BF)


def down(hidden, w):
    rows, out = hidden.shape[0], w.shape[0]
    return pl.pallas_call(
        down_kernel,
        out_shape=jax.ShapeDtypeStruct((rows, out), BF),
        in_specs=[VMEM, VMEM],
        out_specs=VMEM,
        compiler_params=limit(14),
        cost_estimate=pl.CostEstimate(
            flops=2 * rows * out * w.shape[1], bytes_accessed=4 << 20, transcendentals=0
        ),
        name="down",
    )(hidden, w)


def pair_kernel(a_ref, b_ref, out_ref):
    rows = out_ref.shape[1]
    for k in range(out_ref.shape[0]):
        at = slice(k * rows, (k + 1) * rows)
        out_ref[k] = (a_ref[at, :].astype(F32) + b_ref[at, :].astype(F32)).astype(BF)


def pair_sum(a, b):
    return pl.pallas_call(
        pair_kernel,
        out_shape=jax.ShapeDtypeStruct((4, a.shape[0] // 4, a.shape[1]), BF),
        in_specs=[VMEM] * 2,
        out_specs=VMEM,
        compiler_params=limit(4),
        cost_estimate=pl.CostEstimate(flops=10**8, bytes_accessed=1 << 20, transcendentals=0),
        name="pair_sum",
    )(a, b)


def pooled_kernel(x_ref, w_ref, out_ref):
    out_ref[...] = jnp.dot(x_ref[...], w_ref[:, 0:128], preferred_element_type=F32).astype(BF)


def pooled(x, w):
    return pl.pallas_call(
        pooled_kernel,
        out_shape=jax.ShapeDtypeStruct((x.shape[0], 128), BF),
        in_specs=[VMEM] * 2,
        out_specs=VMEM,
        compiler_params=limit(6),
        cost_estimate=pl.CostEstimate(
            flops=2 * x.shape[0] * x.shape[1] * 128, bytes_accessed=2 << 20, transcendentals=0
        ),
        name="pooled",
    )(x, w)


def mixer_kernel(kind_ref, mine_ref, other_ref, w_ref, pool_ref, scale_ref, keep_ref, send_ref):
    rows = 2 * mine_ref.shape[0]
    tile = rows // 8
    kind, core = kind_ref[0], kind_ref[1]
    values = jnp.dot(other_ref[...], w_ref[:, 0:128], preferred_element_type=F32).astype(BF)
    values = jnp.concatenate([mine_ref[...].astype(F32), values.astype(F32)], axis=0)
    in_order = []
    for i in range(4):
        mine = values[i * tile : (i + 1) * tile]
        other = values[(4 + i) * tile : (5 + i) * tile]
        in_order += [jnp.where(core == 0, mine, other), jnp.where(core == 0, other, mine)]
    values = jnp.concatenate(in_order, axis=0)
    place = lax.broadcasted_iota(jnp.int32, (rows, 128), 0) % LEN
    total = values
    chosen = jnp.zeros_like(values)
    for slot in range(4):
        lag = 2**slot
        earlier = jnp.concatenate([jnp.zeros((lag, 128), F32), total[: rows - lag]], axis=0)
        total = total + jnp.where(place >= lag, earlier, 0.0)
        window = 2 * lag
        mean = total / jnp.minimum(place + 1, window).astype(F32)
        chosen = jnp.where(kind == slot, mean, chosen)
    deviation = (chosen - values).astype(BF)
    mixed = jnp.dot(deviation, pool_ref[...], preferred_element_type=F32)
    mixed = mixed * scale_ref[...].astype(F32)
    mixed = by_core(core, [mixed[i * tile : (i + 1) * tile] for i in range(8)]).astype(BF)
    for at in range(0, w_ref.shape[0], 256):
        share = lax.dot_general(
            mixed, w_ref[at : at + 256, 128:256], (((1,), (1,)), ((), ())), preferred_element_type=F32
        ).astype(BF)
        keep_ref[:, at : at + 256] = share[: rows // 2]
        send_ref[:, at : at + 256] = share[rows // 2 :]


def mixer(kind, mine, other, w, pool_w, pool_scale):
    rows, depth = 2 * other.shape[0], other.shape[1]
    return pl.pallas_call(
        mixer_kernel,
        out_shape=(jax.ShapeDtypeStruct((rows // 2, depth), BF),) * 2,
        in_specs=[SMEM] + [VMEM] * 5,
        out_specs=(VMEM, VMEM),
        compiler_params=limit(14),
        cost_estimate=pl.CostEstimate(
            flops=4 * rows * depth * 128, bytes_accessed=4 << 20, transcendentals=0
        ),
        name="mixer",
    )(kind, mine, other, w, pool_w, pool_scale)


X_GROUPS = [[2 * x + core for x in range(4)] for core in range(2)]


def core_swap(array):
    return lax.ppermute(array, "tp", [(k, k ^ 1) for k in range(8)])


def shares_of_rows(mine, other):
    tiles = pair_sum(mine, core_swap(other))
    return lax.all_to_all(tiles, "tp", 0, 0, tiled=True, axis_index_groups=X_GROUPS)


def rows_of_all(copies):
    mine = lax.all_to_all(copies, "tp", 0, 0, tiled=True, axis_index_groups=X_GROUPS)
    mine = mine.reshape(-1, copies.shape[-1])
    return mine, core_swap(mine)


def body(tokens, w_gate, w_up, w_down, w_mix_in, w_mix_out, pool_w, pool_scale, norm_gains):
    tp_size, tp_at = lax.axis_size("tp"), lax.axis_index("tp")
    fs_at = lax.axis_index("fs")
    z, y = fs_at // NY, fs_at % NY
    own_rows = tokens.shape[0] // tp_size
    width = w_gate.shape[1]

    groups = [[k * NY + j for j in range(NY)] for k in range(NZ)]
    second_width = 256 + width
    first, second = pack(w_gate, w_up, w_mix_in, w_mix_out.T, w_down.T)
    first = lax.all_gather(first, "fs", axis=0, tiled=True, axis_index_groups=groups)

    first_block = lax.rem(z + 8, NZ)
    core = lax.rem(tp_at, 2)
    gains = rolled(norm_gains, first_block)
    numbers = jnp.stack([first_block, core, lax.rem(tp_at, 4), y]).astype(jnp.int32)

    first, late_tokens = lax.optimization_barrier((first, tokens))
    back = ahead = jnp.concatenate([first, second], axis=0)
    x = first_norm(numbers[0:2], late_tokens, gains)
    got = {0: back}
    total = None
    for k in range(1, 9):
        if k == 7:
            last_second = shift(back[128:, :second_width], dz=2)
        back = got[-k] = shift(back, dz=1)
        if k < 8:
            ahead = got[k] = shift(ahead, dz=-1)
        places = ([0] if k == 1 else []) + [-k] + ([k] if k < 8 else [])
        total = absorb(x, [got[p] for p in places], tuple(8 + p for p in places), total)
    payloads = [got[k] for k in OFFSETS]

    pieces = []
    for batch in BATCHES:
        own = [last_second if s == -8 else got[s][128:, :second_width] for s in batch]
        own = jnp.concatenate(own, axis=0)
        pieces += [own, shift(own, dy=1), shift(own, dy=2), shift(own, dy=-1)]
    mix_w, down_w = assemble(numbers[3:4], pieces, width)

    stream = lax.dynamic_slice_in_dim(late_tokens, tp_at * own_rows, own_rows, 0)
    stream = rolled(stream, first_block).astype(F32)
    hidden, other = silu(total)
    other, mine = down(other, down_w), down(hidden, down_w)
    parts = shares_of_rows(mine, other)
    stream, copies = settle(parts, stream, gains, 1, 0.5)
    kind = jnp.stack([numbers[2], numbers[1]])
    mine, other = rows_of_all(copies)
    share = mixer(kind, pooled(mine, mix_w), other, mix_w, pool_w[0], pool_scale[None])
    stream, copies = settle(shares_of_rows(*share), stream, gains, 3, 1.0)
    mine, other = rows_of_all(copies)
    hidden, gate_up = gated(mine, payloads, width)
    other = gated(other, [gate_up], width)
    other, mine = down(other, down_w), down(hidden, down_w)
    parts = shares_of_rows(mine, other)
    return finish(numbers[0:1], parts, stream, gains)


def solution(mesh):
    in_specs = (
        P("fs", None),
        P("fs", "tp"),
        P("fs", "tp"),
        P("tp", "fs"),
        P("fs", "tp"),
        P("tp", "fs"),
        P("tp", None, None),
        P("tp"),
        P(),
    )
    out_specs = P(("fs", "tp"), None)

    return jax.shard_map(body, mesh=mesh, in_specs=in_specs, out_specs=out_specs, check_vma=False)
```

```python
import functools

import jax
import jax.numpy as jnp
from jax import lax
from jax.experimental import pallas as pl
from jax.experimental.pallas import tpu as pltpu
from jax.sharding import PartitionSpec as P


LEN = 64
NZ, NY = 16, 4
BF = jnp.bfloat16
F32 = jnp.float32
VMEM = pl.BlockSpec(memory_space=pltpu.VMEM)
SMEM = pl.BlockSpec(memory_space=pltpu.SMEM)


def limit(mib):
    return pltpu.CompilerParams(vmem_limit_bytes=mib * 1024 * 1024)


OFFSETS = tuple(range(-8, 8))
BATCHES = ((0, -1, 1, -2, 2, -3, 3, -4, 4, -5, 5), (-6, 6, -7, 7, -8))
HBM = pl.BlockSpec(memory_space=pltpu.HBM)


def fs_shift(dy, dz):
    return [
        (z * NY + y, ((z + dz) % NZ) * NY + (y + dy) % NY) for z in range(NZ) for y in range(NY)
    ]


def shift(array, dy=0, dz=0):
    return lax.ppermute(array, "fs", fs_shift(dy, dz))


def rolled(array, first_block):
    twice = jnp.concatenate([array, array], axis=1)
    return lax.dynamic_slice_in_dim(twice, first_block * 128, array.shape[1], 1)


def pack_kernel(gate_in, up_in, mix_in, mix_out, down_in, first_ref, second_ref, *scratch):
    held, sems = scratch[:5], scratch[5]
    copies = []
    for k, (src, dst) in enumerate(zip((gate_in, up_in, mix_in, mix_out, down_in), held)):
        copies.append(pltpu.make_async_copy(src, dst, sems.at[k]))
        copies[-1].start()
    for copy in copies:
        copy.wait()
    gate_ref, up_ref, in_ref, out_ref, down_ref = held
    width = gate_ref.shape[1]
    whole = width // 128 * 128
    first_ref[:, :whole] = gate_ref[:, :whole]
    first_ref[:, whole : 2 * whole] = up_ref[:, :whole]
    first_ref[:, 2 * whole :] = jnp.concatenate([gate_ref[:, whole:], up_ref[:, whole:]], axis=1)
    second_ref[:, 0:128] = in_ref[...]
    second_ref[:, 128:256] = out_ref[...]
    second_ref[:, 256 : 256 + width] = down_ref[...]
    second_ref[:, 256 + width :] = jnp.zeros((32, width - 256), BF)


def pack(*weights):
    shape = jax.ShapeDtypeStruct((32, 2 * weights[0].shape[1]), BF)
    return pl.pallas_call(
        pack_kernel,
        out_shape=(shape, shape),
        in_specs=[HBM] * 5,
        out_specs=(VMEM, VMEM),
        scratch_shapes=[pltpu.VMEM(w.shape, BF) for w in weights] + [pltpu.SemaphoreType.DMA((5,))],
        compiler_params=limit(63),
        cost_estimate=pl.CostEstimate(flops=10**8, bytes_accessed=1 << 18, transcendentals=0),
        name="pack",
    )(*weights)


def by_core(core, blocks):
    even, odd = blocks[0::2], blocks[1::2]
    mine = [jnp.where(core == 0, a, b) for a, b in zip(even, odd)]
    other = [jnp.where(core == 0, b, a) for a, b in zip(even, odd)]
    return jnp.concatenate(mine + other, axis=0)


def first_norm_kernel(at_ref, x_ref, gain_ref, out_ref):
    rows, depth = x_ref.shape
    tile = rows // 8
    block, core = at_ref[0], at_ref[1]
    halves = ([], [])
    for i in range(4):
        x0 = x_ref[2 * i * tile : (2 * i + 1) * tile, :].astype(F32)
        x1 = x_ref[(2 * i + 1) * tile : (2 * i + 2) * tile, :].astype(F32)
        for k, x in enumerate((x0, x1)):
            scale = lax.rsqrt(jnp.mean(x * x, axis=-1, keepdims=True) + 1e-06)
            halves[k].append(scale)
    for p in range(depth // 128):
        start = pl.multiple_of(lax.rem(block + p, depth // 128) * 128, 128)
        gain = gain_ref[0:1, p * 128 : (p + 1) * 128]
        mine, other = [], []
        for i in range(4):
            x0 = x_ref[2 * i * tile : (2 * i + 1) * tile, pl.ds(start, 128)].astype(F32)
            x1 = x_ref[(2 * i + 1) * tile : (2 * i + 2) * tile, pl.ds(start, 128)].astype(F32)
            x0 = (x0 * halves[0][i] * gain).astype(BF)
            x1 = (x1 * halves[1][i] * gain).astype(BF)
            mine.append(jnp.where(core == 0, x0, x1))
            other.append(jnp.where(core == 0, x1, x0))
        for i in range(4):
            out_ref[i * tile : (i + 1) * tile, p * 128 : (p + 1) * 128] = mine[i]
            out_ref[(4 + i) * tile : (5 + i) * tile, p * 128 : (p + 1) * 128] = other[i]


def first_norm(at, tokens, gain):
    return pl.pallas_call(
        first_norm_kernel,
        out_shape=jax.ShapeDtypeStruct(tokens.shape, BF),
        in_specs=[SMEM, VMEM, VMEM],
        out_specs=VMEM,
        compiler_params=limit(8),
        cost_estimate=pl.CostEstimate(flops=10**9, bytes_accessed=3 << 20, transcendentals=0),
        name="first_norm",
    )(at, tokens, gain)


def rms_scale(values, gain):
    return values * lax.rsqrt(jnp.mean(values * values, axis=-1, keepdims=True) + 1e-06) * gain


def settle_kernel(factor, row, parts_ref, stream_ref, gain_ref, new_ref, normed_ref):
    total = parts_ref[0].astype(F32)
    for k in range(1, parts_ref.shape[0]):
        total = total + parts_ref[k].astype(F32)
    stream = stream_ref[...] + factor * rms_scale(total, gain_ref[row : row + 1, :])
    new_ref[...] = stream
    normed = rms_scale(stream, gain_ref[row + 1 : row + 2, :]).astype(BF)
    for k in range(normed_ref.shape[0]):
        normed_ref[k] = normed


def settle(parts, stream, gains, row, factor):
    return pl.pallas_call(
        functools.partial(settle_kernel, factor, row),
        out_shape=(
            jax.ShapeDtypeStruct(stream.shape, F32),
            jax.ShapeDtypeStruct((4, *stream.shape), BF),
        ),
        in_specs=[VMEM] * 3,
        out_specs=(VMEM, VMEM),
        compiler_params=limit(6),
        cost_estimate=pl.CostEstimate(flops=10**8, bytes_accessed=1 << 20, transcendentals=0),
        name="settle",
    )(parts, stream, gains)


def finish_kernel(at_ref, parts_ref, stream_ref, gain_ref, out_ref):
    total = parts_ref[0].astype(F32)
    for k in range(1, parts_ref.shape[0]):
        total = total + parts_ref[k].astype(F32)
    result = (stream_ref[...] + 0.5 * rms_scale(total, gain_ref[5:6, :])).astype(BF)
    blocks = result.shape[1] // 128
    for p in range(blocks):
        start = pl.multiple_of(lax.rem(at_ref[0] + p, blocks) * 128, 128)
        out_ref[:, pl.ds(start, 128)] = result[:, p * 128 : (p + 1) * 128]


def finish(at, parts, stream, gains):
    return pl.pallas_call(
        finish_kernel,
        out_shape=jax.ShapeDtypeStruct(stream.shape, BF),
        in_specs=[SMEM] + [VMEM] * 3,
        out_specs=VMEM,
        compiler_params=limit(6),
        cost_estimate=pl.CostEstimate(flops=10**8, bytes_accessed=1 << 20, transcendentals=0),
        name="finish",
    )(at, parts, stream, gains)


def act(gate, up):
    return (gate / (1.0 + jnp.exp(-gate)) * up).astype(BF)


def gated_product(x, w_ref, out_ref):
    width = out_ref.shape[1]
    whole = width // 128 * 128
    at = 0
    while at < whole:
        n = min(256, whole - at)
        gate = jnp.dot(x, w_ref[:, at : at + n], preferred_element_type=F32)
        up = jnp.dot(x, w_ref[:, whole + at : whole + at + n], preferred_element_type=F32)
        out_ref[:, at : at + n] = act(gate, up)
        at += n
    both = jnp.dot(x, w_ref[:, 2 * whole :], preferred_element_type=F32)
    out_ref[:, whole:] = act(both[:, : width - whole], both[:, width - whole :])


def gated_first_kernel(x_ref, *refs):
    payloads, out_ref, w_ref = refs[:NZ], refs[-2], refs[-1]
    for k in range(NZ):
        w_ref[k * 128 : (k + 1) * 128, :] = payloads[k][0:128, :]
    gated_product(x_ref[...], w_ref, out_ref)


def gated_then_kernel(x_ref, w_ref, out_ref):
    gated_product(x_ref[...], w_ref, out_ref)


def gated(x, weights, width):
    rows, depth = x.shape
    hidden = jax.ShapeDtypeStruct((rows, width), BF)
    whole = jax.ShapeDtypeStruct((depth, 2 * width), BF)
    first = len(weights) > 1
    return pl.pallas_call(
        gated_first_kernel if first else gated_then_kernel,
        out_shape=(hidden, whole) if first else hidden,
        in_specs=[VMEM] * (1 + len(weights)),
        out_specs=(VMEM, VMEM) if first else VMEM,
        compiler_params=limit(16 if first else 10),
        cost_estimate=pl.CostEstimate(
            flops=4 * rows * depth * width, bytes_accessed=8 << 20, transcendentals=0
        ),
        name="gated",
    )(x, *weights)


def absorb_kernel(places, x_ref, *refs):
    n = len(places)
    blocks, total_ref = refs[:n], refs[-1]
    x = [x_ref[:, place * 128 : (place + 1) * 128] for place in places]
    x = x[0] if n == 1 else jnp.concatenate(x, axis=1)
    width = total_ref.shape[1]
    for at in range(0, width, 256):
        end = min(width, at + 256)
        w = [block[0:128, at:end] for block in blocks]
        w = w[0] if n == 1 else jnp.concatenate(w, axis=0)
        part = jnp.dot(x, w, preferred_element_type=F32)
        total_ref[:, at:end] = part if len(refs) == n + 1 else refs[n][:, at:end] + part


def absorb(x, blocks, places, total=None):
    rows, width, n = x.shape[0], blocks[0].shape[1], len(blocks)
    carried = () if total is None else (total,)
    return pl.pallas_call(
        functools.partial(absorb_kernel, places),
        out_shape=jax.ShapeDtypeStruct((rows, width), F32),
        in_specs=[VMEM] * (1 + n + len(carried)),
        out_specs=VMEM,
        input_output_aliases={} if total is None else {1 + n: 0},
        compiler_params=limit(6),
        cost_estimate=pl.CostEstimate(
            flops=2 * rows * width * 128 * n, bytes_accessed=n << 19, transcendentals=0
        ),
        name="absorb",
    )(x, *blocks, *carried)


def silu_kernel(total_ref, mine_ref, other_ref):
    half, width = mine_ref.shape
    whole = width // 128 * 128
    for k, ref in enumerate((mine_ref, other_ref)):
        rows = slice(k * half, (k + 1) * half)
        ref[:, :whole] = act(total_ref[rows, :whole], total_ref[rows, whole : 2 * whole])
        both = total_ref[rows, 2 * whole :]
        ref[:, whole:] = act(both[:, : width - whole], both[:, width - whole :])


def silu(total):
    rows, width = total.shape
    return pl.pallas_call(
        silu_kernel,
        out_shape=(jax.ShapeDtypeStruct((rows // 2, width // 2), BF),) * 2,
        in_specs=[VMEM],
        out_specs=(VMEM, VMEM),
        compiler_params=limit(4),
        cost_estimate=pl.CostEstimate(flops=10**8, bytes_accessed=1 << 20, transcendentals=0),
        name="silu",
    )(total)


def assemble_kernel(y_ref, *refs):
    ins, mix_ref, down_ref = refs[:-2], refs[-2], refs[-1]
    y = y_ref[0]
    width = mix_ref.shape[1] + down_ref.shape[1]
    for k, batch in enumerate(BATCHES):
        for j in range(NY):
            owner = lax.rem(y - j + NY, NY)
            src = ins[NY * k + j]
            for i, offset in enumerate(batch):
                start = pl.multiple_of(OFFSETS.index(offset) * 128 + owner * 32, 32)
                mix_ref[pl.ds(start, 32), :] = src[i * 32 : (i + 1) * 32, 0:256]
                down_ref[pl.ds(start, 32), :] = src[i * 32 : (i + 1) * 32, 256:width]


def assemble(y, pieces, down_width):
    rows = NZ * NY * 32
    return pl.pallas_call(
        assemble_kernel,
        out_shape=(
            jax.ShapeDtypeStruct((rows, 256), BF),
            jax.ShapeDtypeStruct((rows, down_width), BF),
        ),
        in_specs=[SMEM] + [VMEM] * len(pieces),
        out_specs=(VMEM, VMEM),
        compiler_params=limit(14),
        cost_estimate=pl.CostEstimate(flops=10**8, bytes_accessed=8 << 20, transcendentals=0),
        name="assemble",
    )(y, *pieces)


def down_kernel(h_ref, w_ref, out_ref):
    h = h_ref[...]
    for at in range(0, w_ref.shape[0], 256):
        out_ref[:, at : at + 256] = lax.dot_general(
            h, w_ref[at : at + 256, :], (((1,), (1,)), ((), ())), preferred_element_type=F32
        ).astype(BF)


def down(hidden, w):
    rows, out = hidden.shape[0], w.shape[0]
    return pl.pallas_call(
        down_kernel,
        out_shape=jax.ShapeDtypeStruct((rows, out), BF),
        in_specs=[VMEM, VMEM],
        out_specs=VMEM,
        compiler_params=limit(14),
        cost_estimate=pl.CostEstimate(
            flops=2 * rows * out * w.shape[1], bytes_accessed=4 << 20, transcendentals=0
        ),
        name="down",
    )(hidden, w)


def pair_kernel(a_ref, b_ref, out_ref):
    rows = out_ref.shape[1]
    for k in range(out_ref.shape[0]):
        at = slice(k * rows, (k + 1) * rows)
        out_ref[k] = (a_ref[at, :].astype(F32) + b_ref[at, :].astype(F32)).astype(BF)


def pair_sum(a, b):
    return pl.pallas_call(
        pair_kernel,
        out_shape=jax.ShapeDtypeStruct((4, a.shape[0] // 4, a.shape[1]), BF),
        in_specs=[VMEM] * 2,
        out_specs=VMEM,
        compiler_params=limit(4),
        cost_estimate=pl.CostEstimate(flops=10**8, bytes_accessed=1 << 20, transcendentals=0),
        name="pair_sum",
    )(a, b)


def pooled_kernel(x_ref, w_ref, out_ref):
    out_ref[...] = jnp.dot(x_ref[...], w_ref[:, 0:128], preferred_element_type=F32).astype(BF)


def pooled(x, w):
    return pl.pallas_call(
        pooled_kernel,
        out_shape=jax.ShapeDtypeStruct((x.shape[0], 128), BF),
        in_specs=[VMEM] * 2,
        out_specs=VMEM,
        compiler_params=limit(6),
        cost_estimate=pl.CostEstimate(
            flops=2 * x.shape[0] * x.shape[1] * 128, bytes_accessed=2 << 20, transcendentals=0
        ),
        name="pooled",
    )(x, w)


def mixer_kernel(kind_ref, mine_ref, other_ref, w_ref, pool_ref, scale_ref, keep_ref, send_ref):
    rows = 2 * mine_ref.shape[0]
    tile = rows // 8
    kind, core = kind_ref[0], kind_ref[1]
    values = jnp.dot(other_ref[...], w_ref[:, 0:128], preferred_element_type=F32).astype(BF)
    values = jnp.concatenate([mine_ref[...].astype(F32), values.astype(F32)], axis=0)
    in_order = []
    for i in range(4):
        mine = values[i * tile : (i + 1) * tile]
        other = values[(4 + i) * tile : (5 + i) * tile]
        in_order += [jnp.where(core == 0, mine, other), jnp.where(core == 0, other, mine)]
    values = jnp.concatenate(in_order, axis=0)
    place = lax.broadcasted_iota(jnp.int32, (rows, 128), 0) % LEN
    total = values
    chosen = jnp.zeros_like(values)
    for slot in range(4):
        lag = 2**slot
        earlier = jnp.concatenate([jnp.zeros((lag, 128), F32), total[: rows - lag]], axis=0)
        total = total + jnp.where(place >= lag, earlier, 0.0)
        window = 2 * lag
        mean = total / jnp.minimum(place + 1, window).astype(F32)
        chosen = jnp.where(kind == slot, mean, chosen)
    deviation = (chosen - values).astype(BF)
    mixed = jnp.dot(deviation, pool_ref[...], preferred_element_type=F32)
    mixed = mixed * scale_ref[...].astype(F32)
    mixed = by_core(core, [mixed[i * tile : (i + 1) * tile] for i in range(8)]).astype(BF)
    keep_ref[...] = mixed[: rows // 2]
    send_ref[...] = mixed[rows // 2 :]


def spread_kernel(m_ref, w_ref, out_ref):
    m = m_ref[...]
    for at in range(0, w_ref.shape[0], 256):
        out_ref[:, at : at + 256] = lax.dot_general(
            m, w_ref[at : at + 256, 128:256], (((1,), (1,)), ((), ())), preferred_element_type=F32
        ).astype(BF)


def spread(mixed, w):
    rows, depth = mixed.shape[0], w.shape[0]
    return pl.pallas_call(
        spread_kernel,
        out_shape=jax.ShapeDtypeStruct((rows, depth), BF),
        in_specs=[VMEM] * 2,
        out_specs=VMEM,
        compiler_params=limit(6),
        cost_estimate=pl.CostEstimate(
            flops=2 * rows * depth * 128, bytes_accessed=2 << 20, transcendentals=0
        ),
        name="spread",
    )(mixed, w)


def mixer(kind, mine, other, w, pool_w, pool_scale):
    rows, depth = 2 * other.shape[0], other.shape[1]
    return pl.pallas_call(
        mixer_kernel,
        out_shape=(jax.ShapeDtypeStruct((rows // 2, 128), BF),) * 2,
        in_specs=[SMEM] + [VMEM] * 5,
        out_specs=(VMEM, VMEM),
        compiler_params=limit(14),
        cost_estimate=pl.CostEstimate(
            flops=4 * rows * depth * 128, bytes_accessed=4 << 20, transcendentals=0
        ),
        name="mixer",
    )(kind, mine, other, w, pool_w, pool_scale)


X_GROUPS = [[2 * x + core for x in range(4)] for core in range(2)]


def core_swap(array):
    return lax.ppermute(array, "tp", [(k, k ^ 1) for k in range(8)])


def shares_of_rows(mine, other):
    tiles = pair_sum(mine, core_swap(other))
    return lax.all_to_all(tiles, "tp", 0, 0, tiled=True, axis_index_groups=X_GROUPS)


def rows_of_all(copies):
    mine = lax.all_to_all(copies, "tp", 0, 0, tiled=True, axis_index_groups=X_GROUPS)
    mine = mine.reshape(-1, copies.shape[-1])
    return mine, core_swap(mine)


def body(tokens, w_gate, w_up, w_down, w_mix_in, w_mix_out, pool_w, pool_scale, norm_gains):
    tp_size, tp_at = lax.axis_size("tp"), lax.axis_index("tp")
    fs_at = lax.axis_index("fs")
    z, y = fs_at // NY, fs_at % NY
    own_rows = tokens.shape[0] // tp_size
    width = w_gate.shape[1]

    groups = [[k * NY + j for j in range(NY)] for k in range(NZ)]
    second_width = 256 + width
    first, second = pack(w_gate, w_up, w_mix_in, w_mix_out.T, w_down.T)
    first = lax.all_gather(first, "fs", axis=0, tiled=True, axis_index_groups=groups)

    first_block = lax.rem(z + 8, NZ)
    core = lax.rem(tp_at, 2)
    gains = rolled(norm_gains, first_block)
    numbers = jnp.stack([first_block, core, lax.rem(tp_at, 4), y]).astype(jnp.int32)

    first, late_tokens = lax.optimization_barrier((first, tokens))
    back = ahead = jnp.concatenate([first, second], axis=0)
    x = first_norm(numbers[0:2], late_tokens, gains)
    got = {0: back}
    total = None
    for k in range(1, 9):
        if k == 7:
            last_second = shift(back[128:, :second_width], dz=2)
        back = got[-k] = shift(back, dz=1)
        if k < 8:
            ahead = got[k] = shift(ahead, dz=-1)
        places = ([0] if k == 1 else []) + [-k] + ([k] if k < 8 else [])
        total = absorb(x, [got[p] for p in places], tuple(8 + p for p in places), total)
    payloads = [got[k] for k in OFFSETS]

    pieces = []
    for batch in BATCHES:
        own = [last_second if s == -8 else got[s][128:, :second_width] for s in batch]
        own = jnp.concatenate(own, axis=0)
        pieces += [own, shift(own, dy=1), shift(own, dy=2), shift(own, dy=-1)]
    mix_w, down_w = assemble(numbers[3:4], pieces, width)

    stream = lax.dynamic_slice_in_dim(late_tokens, tp_at * own_rows, own_rows, 0)
    stream = rolled(stream, first_block).astype(F32)
    hidden, other = silu(total)
    other, mine = down(other, down_w), down(hidden, down_w)
    parts = shares_of_rows(mine, other)
    stream, copies = settle(parts, stream, gains, 1, 0.5)
    kind = jnp.stack([numbers[2], numbers[1]])
    mine, other = rows_of_all(copies)
    mine = pooled(mine, mix_w)
    mine, other = mixer(kind, mine, other, mix_w, pool_w[0], pool_scale[None])
    other, mine = spread(other, mix_w), spread(mine, mix_w)
    stream, copies = settle(shares_of_rows(mine, other), stream, gains, 3, 1.0)
    mine, other = rows_of_all(copies)
    hidden, gate_up = gated(mine, payloads, width)
    other = gated(other, [gate_up], width)
    other, mine = down(other, down_w), down(hidden, down_w)
    parts = shares_of_rows(mine, other)
    return finish(numbers[0:1], parts, stream, gains)


def solution(mesh):
    in_specs = (
        P("fs", None),
        P("fs", "tp"),
        P("fs", "tp"),
        P("tp", "fs"),
        P("fs", "tp"),
        P("tp", "fs"),
        P("tp", None, None),
        P("tp"),
        P(),
    )
    out_specs = P(("fs", "tp"), None)

    return jax.shard_map(body, mesh=mesh, in_specs=in_specs, out_specs=out_specs, check_vma=False)
```
